32 devices in a mesh: ep: 8 (over z, core), tp: 4 (over y, x).
Axes of the slice: x: 2, y: 2, z: 4, core: 2. Of those that a mesh axis runs over, the one named last changes fastest.
Arguments:
- tokens: bfloat16 [1024, 2048], P('ep'), may hold values from -6 to 6
- cotangent: bfloat16 [1024, 2048], P('ep'), may hold values from -6 to 6
- routes: int32 [1024, 2], P('ep'), may hold values from 0 to 7, all different within a row; in each aligned block of 128 rows (0 to 127, 128 to 255, ...) at most 64 rows name the same one
- route_weight: float32 [1024, 2], P('ep'), may hold values from 0.1 to 1
- w_gate: bfloat16 [8, 2048, 1024], P('ep', None, 'tp'), may hold values from -0.1875 to 0.1875
- w_up: bfloat16 [8, 2048, 1024], P('ep', None, 'tp'), may hold values from -0.1875 to 0.1875
- w_down: bfloat16 [8, 1024, 2048], P('ep', 'tp'), may hold values from -0.1875 to 0.1875
Outputs:
- grad_tokens: bfloat16 [1024, 2048], P('ep', 'tp')
- grad_route_weight: float32 [1024, 2], P('ep')
- grad_gate: float32 [8, 2048, 1024], P('ep', None, 'tp')
- grad_up: float32 [8, 2048, 1024], P('ep', None, 'tp')
- grad_down: float32 [8, 1024, 2048], P('ep', 'tp')
The draws below stay inside these ranges and needn't reach their ends.
Inputs may be any that keep to these rules, and one draw needn't show every extreme that they name: `routes`: each row names 2 different experts. In each aligned block of 128 rows (the rows of one index of ep) no expert is named by more than 64 rows, and in every draw some expert is named by exactly 64 rows of some block.
All inputs are finite; a program needn't handle non-finite values.
Results may differ from the reference program's by a relative error of at most 0.023.
Values may be sent and summed in bfloat16 or wider, within the bound.
No kernel may reach another device: no remote copies, remote signals or barrier semaphores. Data moves between devices by JAX's collectives and lax.ppermute only.
A program may use at most 64 MiB of HBM per device.

```python
import math
import jax
import jax.numpy as jnp
import numpy as np
from jax import lax

D = 2048
FF = 1024
TOP_K = 2
TOK_DEV = 128
EXPERTS = 8
TOKENS = 1024
CAP = 64
N_EP = 8
N_TP = 4


def strengthened(result, rng, source, target, blocks, factor):
    def block_of(axis_at):
        return (jnp.arange(result.shape[axis_at]) // (result.shape[axis_at] // blocks)).reshape((-1,) + (1,) * (result.ndim - 1 - axis_at))

    near = jax.random.permutation(rng, blocks)[block_of(target)]
    second = (block_of(target) + blocks // 2) % blocks
    return jnp.where((block_of(source) == near) | (block_of(source) == second), factor * result, result)


def levels(rng, shape, cuts, least, top_value):
    def one(dim, shards_of):
        heights = jax.random.uniform(jax.random.fold_in(jax.random.fold_in(rng, 6), dim), (shards_of,), jnp.float32, least / len(cuts), top_value / len(cuts))
        return jnp.repeat(jnp.exp(heights), shape[dim] // shards_of).reshape((-1,) + (1,) * (len(shape) - dim - 1))

    gain = one(*cuts[0])
    for cut in cuts[1:]:
        gain = gain * one(*cut)
    return gain


def routed_block(own_key, own, number, rows, amount, top, bound, slope):
    ranking = jax.random.permutation(own_key, amount)
    packed, common = shares(amount, rows * top, bound, slope, True), shares(amount, rows * top, bound, slope, False)
    places = jnp.arange(amount)

    def named(lengths, rotation):
        used = int((lengths > 0).sum())
        fixed = max(1, used // 4)
        moved = fixed + (places - fixed + rotation * (used - fixed)) % max(1, amount - fixed)
        return jnp.zeros((amount,), jnp.int32).at[ranking[jnp.where(places < fixed, places, moved)]].set(jnp.asarray(lengths, jnp.int32))

    lengths = jnp.where(number % 4 == 0, named(packed, number // 4), named(common, number - number // 4 - 1))
    mixed = jax.random.permutation(jax.random.fold_in(own, 3), amount)
    giver, receiver = mixed[0:amount // 2 * 2:2], mixed[1:amount // 2 * 2:2]
    slack = jnp.minimum(lengths[giver] - 1, bound - lengths[receiver]) // 2
    slack = jnp.where((giver == ranking[0]) | (receiver == ranking[0]) | (lengths[receiver] == 0), 0, jnp.maximum(slack, 0))
    moved = jax.random.randint(jax.random.fold_in(own, 4), (amount // 2,), 0, 1 << 20) % (slack + 1)
    lengths = lengths.at[giver].add(-moved).at[receiver].add(moved)
    members = jnp.searchsorted(jnp.cumsum(lengths), jnp.arange(rows * top), side="right").astype(jnp.int32)
    grid = members.reshape(top, rows).T
    grid = grid[jax.random.permutation(jax.random.fold_in(own, 1), rows)]
    rotation = jax.random.randint(jax.random.fold_in(own, 2), (rows, 1), 0, top)
    return jnp.take_along_axis(grid, (jnp.arange(top)[None, :] + rotation) % top, axis=1)


def shares(number_of, total, bound, lean, full):
    portions = [(1 << 20) // math.isqrt(grade ** lean) + 1 for grade in range(1, number_of + 1)]
    largest = bound if full else min(bound, max(-(-total // number_of), total * portions[0] // sum(portions)))
    least = 1 if total - largest >= number_of - 1 else 0
    holding, surplus = [largest] + [least] * (number_of - 1), total - largest - least * (number_of - 1)
    while surplus > 0:
        free = [i for i in range(1, number_of) if holding[i] < largest] or [i for i in range(1, number_of) if holding[i] < bound]
        pool, budget = sum([portions[i] for i in free]), surplus
        for i in free:
            extra = min(bound - holding[i], max(1, budget * portions[i] // pool), surplus)
            holding[i] = holding[i] + extra
            surplus = surplus - extra
    return np.array(holding)


def scatter_about(stream_key, shape, scale, reach, cuts=(), kind=jnp.bfloat16):
    array = jax.random.normal(stream_key, shape, jnp.float32) * scale
    if len(cuts) > 0:
        array = levels(stream_key, shape, cuts, -0.22, 0.18) * array
    return jnp.clip(array, min=-reach, max=reach).astype(kind)


def gaussian_with(stream_key, shape, spread, reach, shards, heavy, held_as=jnp.bfloat16):
    entries = spread * jax.random.normal(stream_key, shape, jnp.float32)
    if shards:
        entries = entries * levels(stream_key, shape, shards, -0.22, 0.18)
    return jnp.clip(strengthened(entries, jax.random.fold_in(stream_key, 3), *heavy), -reach, reach).astype(held_as)


def setup_inputs(seed: int = 0) -> dict:
    key_list = jax.random.split(jax.random.key(seed), 8)
    tokens = scatter_about(key_list[0], (TOKENS, D), 1.0, 6.0, ((0, 8),))
    cotangent = scatter_about(key_list[1], (TOKENS, D), 1.0, 6.0, ((0, 8),))
    routes_keys = jax.random.split(jax.random.fold_in(key_list[2], 1), TOKENS // TOK_DEV)
    routes_turns = jax.random.permutation(jax.random.fold_in(key_list[2], 3), TOKENS // TOK_DEV)
    routes = jax.vmap(lambda own, number: routed_block(jax.random.fold_in(key_list[2], 2), own, number, TOK_DEV, EXPERTS, TOP_K, CAP, 2))(routes_keys, routes_turns).reshape((TOKENS, TOP_K))
    route_weight = jnp.clip(0.1 + 0.9 * jax.random.uniform(key_list[3], (TOKENS, TOP_K), jnp.float32) ** levels(key_list[3], (TOKENS, TOP_K), ((0, 8),), -0.2, 0.2), 0.1, 1.0)
    w_gate = gaussian_with(key_list[4], (EXPERTS, D, FF), D ** -0.5, 0.1875, ((0, 8), (2, 4)), (2, 1, 4, 2.0))
    w_up = gaussian_with(key_list[5], (EXPERTS, D, FF), D ** -0.5, 0.1875, ((0, 8), (2, 4)), (2, 1, 4, 2.0))
    w_down = scatter_about(key_list[6], (EXPERTS, FF, D), FF ** -0.5, 0.1875, ((0, 8), (1, 4)))
    return {"tokens": tokens, "cotangent": cotangent, "routes": routes, "route_weight": route_weight, "w_gate": w_gate, "w_up": w_up, "w_down": w_down}


def slot_index(block_routes, experts, capacity):
    flat_ids = block_routes.reshape(-1)
    onehot = (flat_ids[:, None] == jnp.arange(experts, dtype=jnp.int32)[None, :]).astype(jnp.int32)
    earlier = jnp.cumsum(onehot, axis=0) - onehot
    return flat_ids * capacity + jnp.sum(earlier * onehot, axis=1)


def expert_grads(inputs):
    rows_x, rows_dy, rows_w, gate_w, up_w, down_w = inputs
    f32 = jnp.float32
    n_rows, model_width = rows_x.shape
    gate_pre = jnp.dot(rows_x, gate_w, preferred_element_type=f32)
    up_pre = jnp.dot(rows_x, up_w, preferred_element_type=f32)
    gate_sig = jax.nn.sigmoid(gate_pre)
    act_full = gate_pre * gate_sig * up_pre
    act = act_full.astype(jnp.bfloat16)
    back_hidden = jnp.dot(rows_dy, down_w.T, preferred_element_type=f32)
    weighted_cot = (rows_w[:, None] * rows_dy.astype(f32)).astype(jnp.bfloat16)
    d_hidden = rows_w[:, None] * back_hidden
    d_gate = (d_hidden * up_pre * gate_sig * (1.0 + gate_pre * (1.0 - gate_sig))).astype(jnp.bfloat16)
    d_up = (d_hidden * gate_pre * gate_sig).astype(jnp.bfloat16)
    gate_grad = jnp.sum(act_full * back_hidden, axis=1)
    pieces = jnp.einsum('rjf,djf->jrd', d_gate.astype(f32).reshape(n_rows, N_TP, -1),
                        gate_w.astype(f32).reshape(model_width, N_TP, -1), precision=lax.Precision.HIGHEST)
    pieces = pieces + jnp.einsum('rjf,djf->jrd', d_up.astype(f32).reshape(n_rows, N_TP, -1),
                                 up_w.astype(f32).reshape(model_width, N_TP, -1), precision=lax.Precision.HIGHEST)
    rounded = lax.optimization_barrier(pieces.astype(jnp.bfloat16))
    route_grad = jnp.sum(rounded.astype(f32), axis=0).astype(jnp.bfloat16)
    grad_gate_e = jnp.dot(rows_x.T, d_gate, preferred_element_type=f32)
    grad_up_e = jnp.dot(rows_x.T, d_up, preferred_element_type=f32)
    grad_down_e = jnp.dot(act.T, weighted_cot, preferred_element_type=f32)
    return route_grad, gate_grad, grad_gate_e, grad_up_e, grad_down_e


def reference(tokens, cotangent, routes, route_weight, w_gate, w_up, w_down):
    f32 = jnp.float32
    blocks = routes.reshape(N_EP, TOK_DEV, TOP_K)
    slot_ids = jax.vmap(lambda block: slot_index(block, EXPERTS, CAP))(blocks)
    expert_ids = blocks.reshape(N_EP, TOK_DEV * TOP_K)
    positions = slot_ids - expert_ids * CAP
    sources = jnp.arange(N_EP, dtype=jnp.int32)[:, None]
    rows_x = jnp.repeat(tokens.reshape(N_EP, TOK_DEV, D), TOP_K, axis=1)
    rows_dy = jnp.repeat(cotangent.reshape(N_EP, TOK_DEV, D), TOP_K, axis=1)
    rows_w = route_weight.reshape(N_EP, TOK_DEV * TOP_K)
    buf_x = jnp.zeros((EXPERTS, N_EP, CAP, D), jnp.bfloat16).at[expert_ids, sources, positions].set(rows_x)
    buf_dy = jnp.zeros((EXPERTS, N_EP, CAP, D), jnp.bfloat16).at[expert_ids, sources, positions].set(rows_dy)
    buf_w = jnp.zeros((EXPERTS, N_EP, CAP), f32).at[expert_ids, sources, positions].set(rows_w)
    recv_rows = N_EP * CAP
    outs = lax.map(expert_grads, (buf_x.reshape(EXPERTS, recv_rows, D), buf_dy.reshape(EXPERTS, recv_rows, D),
                                  buf_w.reshape(EXPERTS, recv_rows), w_gate, w_up, w_down))
    route_grad, gate_grad, grad_gate, grad_up, grad_down = outs
    back_index = sources * CAP + positions
    picked = route_grad[expert_ids, back_index].astype(f32).reshape(TOKENS, TOP_K, D)
    grad_tokens = jnp.sum(picked, axis=1).astype(jnp.bfloat16)
    grad_route_weight = gate_grad[expert_ids, back_index].reshape(TOKENS, TOP_K)
    return grad_tokens, grad_route_weight, grad_gate, grad_up, grad_down
```

```python
import functools

import jax
import jax.numpy as jnp
from jax import lax
from jax.experimental import pallas as pl
from jax.experimental.pallas import tpu as pltpu
from jax.sharding import PartitionSpec as P


F32 = jnp.float32
BF16 = jnp.bfloat16
VMEM = pl.BlockSpec(memory_space=pltpu.VMEM)


def dot(a, b, ca, cb):
    return lax.dot_general(a, b, (((ca,), (cb,)), ((), ())), preferred_element_type=F32)


def place_kernel(n_ep, n_tp, cap, x_ref, dy_ref, routes_ref, weight_ref, place_ref, near_ref, *far_refs):
    toks, width = x_ref.shape
    block = width // n_tp
    me, mine = lax.axis_index("ep"), lax.axis_index("tp")
    ids = routes_ref[...]
    gains = weight_ref[...]
    names = lax.broadcasted_iota(jnp.int32, (toks, n_ep), 1)
    chosen = jnp.zeros((toks, n_ep), F32)
    gain = jnp.zeros((toks, n_ep), F32)
    for k in range(ids.shape[1]):
        hit = ids[:, k : k + 1] == names
        chosen = chosen + jnp.where(hit, 1.0, 0.0)
        gain = gain + jnp.where(hit, gains[:, k : k + 1], 0.0)
    row = lax.broadcasted_iota(jnp.int32, (toks, toks), 0)
    col = lax.broadcasted_iota(jnp.int32, (toks, toks), 1)
    earlier = jnp.where(row < col, 1.0, 0.0).astype(BF16)
    same = jnp.where(row == col, 1.0, 0.0)
    rank = dot(chosen.astype(BF16), earlier, 0, 0)
    chosen_t = dot(chosen.astype(BF16), same.astype(BF16), 0, 0)
    gain_t = lax.dot_general(
        gain, same, (((0,), (0,)), ((), ())), preferred_element_type=F32, precision=lax.Precision.HIGHEST
    )
    slot = lax.broadcasted_iota(jnp.int32, (cap, toks), 0).astype(F32)
    scales = []
    for d in range(n_ep):
        hit = (rank[d : d + 1, :] == slot) & (chosen_t[d : d + 1, :] > 0.5)
        place_ref[d] = jnp.where(hit, 1.0, 0.0).astype(BF16)
        gain_ref_row = jnp.where(hit, gain_t[d : d + 1, :], 0.0)
        scales.append(jnp.sum(gain_ref_row, axis=1, keepdims=True))

    def scale_of(target):
        out = scales[0]
        for d in range(1, n_ep):
            out = jnp.where(target == d, scales[d], out)
        return out

    def pack(target, columns):
        pick = place_ref[target]
        rows_x = dot(pick, x_ref[:, columns], 1, 0).astype(BF16)
        rows_dy = (dot(pick, dy_ref[:, columns], 1, 0) * scale_of(target)).astype(BF16)
        return rows_x, rows_dy

    for q in range(2, n_ep):
        rows_x, rows_dy = pack(me ^ q, pl.ds(pl.multiple_of(mine * block, block), block))
        far_refs[q - 2][:, :block] = rows_x
        far_refs[q - 2][:, block:] = rows_dy
    for q in range(2):
        for r in range(n_tp):
            rows_x, rows_dy = pack(me ^ q, pl.ds(pl.multiple_of((mine ^ r) * block, block), block))
            near_ref[q, r, :, :block] = rows_x
            near_ref[q, r, :, block:] = rows_dy


def expert_kernel(n_tp, *refs):
    g_refs = refs[:n_tp]
    wg_ref, wu_ref, wd_ref, tok_ref, dg_ref, du_ref, act_ref, part_ref = refs[n_tp:]
    block = wg_ref.shape[0] // n_tp
    mine = lax.axis_index("tp")
    offs = [pl.ds(pl.multiple_of((mine ^ r) * block, block), block) for r in range(n_tp)]
    gate = up = back = None
    for r in range(n_tp):
        x = g_refs[r][:, :block]
        dy = g_refs[r][:, block:]
        g = dot(x, wg_ref[offs[r], :], 1, 0)
        u = dot(x, wu_ref[offs[r], :], 1, 0)
        b = dot(dy, wd_ref[:, offs[r]], 1, 1)
        gate, up, back = (g, u, b) if r == 0 else (gate + g, up + u, back + b)
    sig = 1.0 / (1.0 + jnp.exp(-gate))
    silu = gate * sig
    act_full = silu * up
    act_ref[...] = act_full.astype(BF16)
    part_ref[...] = jnp.sum(act_full * back, axis=1, keepdims=True)
    d_gate = (back * up * sig * (1.0 + gate * (1.0 - sig))).astype(BF16)
    d_up = (back * silu).astype(BF16)
    dg_ref[...] = d_gate
    du_ref[...] = d_up
    for r in range(n_tp):
        tok = dot(d_gate, wg_ref[offs[r], :], 1, 1) + dot(d_up, wu_ref[offs[r], :], 1, 1)
        tok_ref[r] = tok.astype(BF16)


def expert_call(blocks, wg, wu, wd):
    n_tp = len(blocks)
    rows = blocks[0].shape[0]
    width, hidden = wg.shape
    return pl.pallas_call(
        functools.partial(expert_kernel, n_tp),
        out_shape=(
            jax.ShapeDtypeStruct((n_tp, rows, width // n_tp), BF16),
            jax.ShapeDtypeStruct((rows, hidden), BF16),
            jax.ShapeDtypeStruct((rows, hidden), BF16),
            jax.ShapeDtypeStruct((rows, hidden), BF16),
            jax.ShapeDtypeStruct((rows, 1), F32),
        ),
        in_specs=[VMEM] * (n_tp + 3),
        out_specs=(VMEM,) * 5,
        cost_estimate=pl.CostEstimate(
            flops=10 * rows * width * hidden,
            bytes_accessed=6 * width * hidden + 6 * rows * width,
            transcendentals=rows * hidden,
        ),
        name="expert",
    )(*blocks, wg, wu, wd)


def weight_kernel(n_tp, n_chunks, pos_ref, *refs):
    g_refs = refs[: n_tp * n_chunks]
    h_refs = refs[n_tp * n_chunks : n_tp * n_chunks + 3 * n_chunks]
    gg_ref, gu_ref, gd_ref = refs[n_tp * n_chunks + 3 * n_chunks :]
    block = gg_ref.shape[1]
    for r in range(n_tp):

        @pl.when(pl.program_id(0) == r)
        def _():
            gg = gu = gd = None
            for i in range(n_chunks):
                x = g_refs[i * n_tp + r][:, :block]
                dy = g_refs[i * n_tp + r][:, block:]
                d_gate, d_up, act = (h_refs[3 * i + k][...] for k in range(3))
                a, b, c = dot(x, d_gate, 0, 0), dot(x, d_up, 0, 0), dot(act, dy, 0, 0)
                gg, gu, gd = (a, b, c) if i == 0 else (gg + a, gu + b, gd + c)
            gg_ref[0] = gg
            gu_ref[0] = gu
            gd_ref[0] = gd


def weight_call(chunks, hiddens, width):
    n_tp = len(chunks[0])
    rows = sum(c[0].shape[0] for c in chunks)
    hidden = hiddens[0][0].shape[1]
    block = width // n_tp
    position = lax.axis_index("tp").astype(jnp.int32).reshape(1)
    return pl.pallas_call(
        functools.partial(weight_kernel, n_tp, len(chunks)),
        out_shape=(
            jax.ShapeDtypeStruct((1, width, hidden), F32),
            jax.ShapeDtypeStruct((1, width, hidden), F32),
            jax.ShapeDtypeStruct((1, hidden, width), F32),
        ),
        grid_spec=pltpu.PrefetchScalarGridSpec(
            num_scalar_prefetch=1,
            grid=(n_tp,),
            in_specs=[VMEM] * (len(chunks) * (n_tp + 3)),
            out_specs=(
                pl.BlockSpec((1, block, hidden), lambda i, pos: (0, pos[0] ^ i, 0)),
                pl.BlockSpec((1, block, hidden), lambda i, pos: (0, pos[0] ^ i, 0)),
                pl.BlockSpec((1, hidden, block), lambda i, pos: (0, 0, pos[0] ^ i)),
            ),
        ),
        cost_estimate=pl.CostEstimate(
            flops=6 * rows * width * hidden, bytes_accessed=12 * width * hidden + 4 * rows * width, transcendentals=0
        ),
        name="weights",
    )(position, *[b for c in chunks for b in c], *[h for hs in hiddens for h in hs])


def collect_kernel(n_ep, place_ref, routes_ref, weight_ref, part_ref, *refs):
    back_refs, (tok_ref, rw_ref) = refs[:n_ep], refs[n_ep:]
    me = lax.axis_index("ep")
    total = None
    for q in range(n_ep):
        rows = dot(place_ref[me ^ q], back_refs[q][...], 0, 0)
        total = rows if q == 0 else total + rows
    tok_ref[...] = total.astype(BF16)
    ids = routes_ref[...]
    n_tp = part_ref.shape[1]
    cap = place_ref.shape[1]
    columns = []
    grads = jnp.zeros(ids.shape, F32)
    names = ids
    for d in range(n_ep):
        line = part_ref[d, 0:1, :].astype(F32)
        for r in range(1, n_tp):
            line = line + part_ref[d, r : r + 1, :].astype(F32)
        hi = line[:, :cap].astype(BF16)
        lo = (line[:, :cap] - hi.astype(F32)).astype(BF16)
        pick = place_ref[d]
        column = dot(pick, hi, 0, 1) + dot(pick, lo, 0, 1)
        grads = grads + jnp.where(names == d, column, 0.0)
    rw_ref[...] = grads / weight_ref[...]


def aligned(tokens, cotangent, routes, route_weight, w_gate, w_up, w_down):
    toks, width = tokens.shape
    n_ep, n_tp = lax.axis_size("ep"), lax.axis_size("tp")
    cap = 2 * toks * routes.shape[1] // n_ep
    block = width // n_tp
    wg, wu, wd = w_gate[0], w_up[0], w_down[0]
    place, near, *far = pl.pallas_call(
        functools.partial(place_kernel, n_ep, n_tp, cap),
        out_shape=(
            jax.ShapeDtypeStruct((n_ep, cap, toks), BF16),
            jax.ShapeDtypeStruct((2, n_tp, cap, 2 * block), BF16),
            *[jax.ShapeDtypeStruct((cap, 2 * block), BF16)] * (n_ep - 2),
        ),
        in_specs=[VMEM] * 4,
        out_specs=(VMEM,) * n_ep,
        name="place",
    )(tokens, cotangent, routes, route_weight)

    def over(axis, size, value, q):
        return lax.ppermute(value, axis, [(i, i ^ q) for i in range(size)])

    partner = over("ep", n_ep, near[1], 1)
    got = {q: over("ep", n_ep, far[q - 2], q) for q in range(2, n_ep)}
    chunks = []
    for first in range(0, n_ep, 2):
        if first == 0:
            both = jnp.concatenate([near[0], partner], axis=1)
            chunks.append([both[r] for r in range(n_tp)])
        else:
            both = jnp.concatenate([got[first], got[first + 1]], axis=0)
            chunks.append([both] + [over("tp", n_tp, both, r) for r in range(1, n_tp)])
    back, hiddens, parts = {}, [], {}
    for i, blocks in enumerate(chunks):
        tok, d_gate, d_up, act, part = expert_call(blocks, wg, wu, wd)
        hiddens.append((d_gate, d_up, act))
        total = tok[0].astype(F32)
        for r in range(1, n_tp):
            total = total + over("tp", n_tp, tok[r], r).astype(F32)
        total = total.astype(BF16)
        for h in range(2):
            q = 2 * i + h
            rows = total[h * cap : (h + 1) * cap]
            back[q] = over("ep", n_ep, rows, q) if q else rows
            parts[q] = part[h * cap : (h + 1) * cap, 0]
    me = lax.axis_index("ep")
    by_offset = jnp.stack([parts[q] for q in range(n_ep)])
    order = me ^ jnp.arange(n_ep)
    by_source = by_offset[order]
    lanes = jnp.zeros((n_ep, n_tp, 128), BF16).at[:, :, :cap].set(by_source[:, None, :].astype(BF16))
    shared = lax.all_to_all(lanes.reshape(n_ep * n_tp, 128), ("ep", "tp"), 0, 0, tiled=True)
    grad_gate, grad_up, grad_down = weight_call(chunks, hiddens, width)
    grad_tokens, grad_route_weight = pl.pallas_call(
        functools.partial(collect_kernel, n_ep),
        out_shape=(
            jax.ShapeDtypeStruct((toks, block), BF16),
            jax.ShapeDtypeStruct(routes.shape, F32),
        ),
        in_specs=[VMEM] * (4 + n_ep),
        out_specs=(VMEM, VMEM),
        name="collect",
    )(place, routes, route_weight, shared.reshape(n_ep, n_tp, 128), *[back[q] for q in range(n_ep)])
    return grad_tokens, grad_route_weight, grad_gate, grad_up, grad_down


def slot_index(block_routes, experts, capacity):
    flat_ids = block_routes.reshape(-1)
    onehot = (flat_ids[:, None] == jnp.arange(experts, dtype=jnp.int32)[None, :]).astype(jnp.int32)
    earlier = jnp.cumsum(onehot, axis=0) - onehot
    return flat_ids * capacity + jnp.sum(earlier * onehot, axis=1)


def general(tokens, cotangent, routes, route_weight, w_gate, w_up, w_down):
    f32 = jnp.float32
    tok_rows, model_width = tokens.shape
    choices_row = routes.shape[1]
    experts = lax.axis_size("ep")
    capacity = 2 * tok_rows * choices_row // experts
    recv_rows = experts * capacity
    slot_ids = slot_index(routes, experts, capacity)

    def exchange(value):
        return lax.all_to_all(value, "ep", split_axis=0, concat_axis=0, tiled=True)

    send_w = jnp.zeros((recv_rows,), f32).at[slot_ids].set(route_weight.reshape(-1))
    empty = jnp.zeros((recv_rows, model_width), jnp.bfloat16)
    send_x = empty.at[slot_ids].set(jnp.repeat(tokens, choices_row, axis=0))
    send_dy = empty.at[slot_ids].set(jnp.repeat(cotangent, choices_row, axis=0))
    rows_x = exchange(send_x.reshape(experts, capacity, model_width)).reshape(recv_rows, model_width)
    rows_dy = exchange(send_dy.reshape(experts, capacity, model_width)).reshape(recv_rows, model_width)
    rows_w = exchange(send_w.reshape(experts, capacity, 1).astype(jnp.bfloat16)).astype(f32).reshape(recv_rows)
    gate_w = w_gate[0]
    up_w = w_up[0]
    down_w = w_down[0]
    gate_pre = jnp.dot(rows_x, gate_w, preferred_element_type=f32)
    up_pre = jnp.dot(rows_x, up_w, preferred_element_type=f32)
    gate_sig = jax.nn.sigmoid(gate_pre)
    act_full = gate_pre * gate_sig * up_pre
    act = act_full.astype(jnp.bfloat16)
    back_hidden = jnp.einsum("rd,fd->rf", rows_dy, down_w, preferred_element_type=f32)
    weighted_cot = (rows_w[:, None] * rows_dy.astype(f32)).astype(jnp.bfloat16)
    d_hidden = rows_w[:, None] * back_hidden
    d_gate = (d_hidden * up_pre * gate_sig * (1.0 + gate_pre * (1.0 - gate_sig))).astype(jnp.bfloat16)
    d_up = (d_hidden * gate_pre * gate_sig).astype(jnp.bfloat16)
    gate_part = jnp.sum(act_full * back_hidden, axis=1)
    token_part = jnp.einsum("rf,df->rd", d_gate, gate_w, preferred_element_type=f32)
    token_part = token_part + jnp.einsum("rf,df->rd", d_up, up_w, preferred_element_type=f32)
    grad_gate = jnp.einsum("rd,rf->df", rows_x, d_gate, preferred_element_type=f32)[None]
    grad_up = jnp.einsum("rd,rf->df", rows_x, d_up, preferred_element_type=f32)[None]
    grad_down = jnp.einsum("rf,rd->fd", act, weighted_cot, preferred_element_type=f32)[None]
    shares = lax.psum_scatter(token_part.astype(jnp.bfloat16), "tp", scatter_dimension=1, tiled=True)
    gate_total = lax.psum(gate_part, "tp")
    back_x = exchange(shares.reshape(experts, capacity, -1))
    back_gate = exchange(gate_total.reshape(experts, capacity).astype(jnp.bfloat16)).astype(f32)
    picked = back_x.reshape(recv_rows, -1)[slot_ids].astype(f32).reshape(tok_rows, choices_row, -1)
    grad_route_weight = back_gate.reshape(recv_rows)[slot_ids].reshape(tok_rows, choices_row)
    grad_tokens = jnp.sum(picked, axis=1).astype(jnp.bfloat16)
    return (grad_tokens, grad_route_weight, grad_gate, grad_up, grad_down)


def on_device(tokens, cotangent, routes, route_weight, w_gate, w_up, w_down):
    n_ep, n_tp = lax.axis_size("ep"), lax.axis_size("tp")
    toks, width = tokens.shape
    cap = 2 * toks * routes.shape[1] // n_ep
    tiles = width % (128 * n_tp) == 0 and w_gate.shape[2] % 128 == 0 and cap % 16 == 0 and cap <= 128
    powers = n_ep & (n_ep - 1) == 0 and n_tp & (n_tp - 1) == 0 and n_ep > 1
    path = aligned if tiles and powers else general
    return path(tokens, cotangent, routes, route_weight, w_gate, w_up, w_down)


def solution(mesh):
    return jax.shard_map(
        on_device,
        mesh=mesh,
        in_specs=(
            P("ep", None),
            P("ep", None),
            P("ep", None),
            P("ep", None),
            P("ep", None, "tp"),
            P("ep", None, "tp"),
            P("ep", "tp", None),
        ),
        out_specs=(
            P("ep", "tp"),
            P("ep", None),
            P("ep", None, "tp"),
            P("ep", None, "tp"),
            P("ep", "tp", None),
        ),
        check_vma=False,
    )
```

```python
import functools

import jax
import jax.numpy as jnp
from jax import lax
from jax.experimental import pallas as pl
from jax.experimental.pallas import tpu as pltpu
from jax.sharding import PartitionSpec as P


F32 = jnp.float32
BF16 = jnp.bfloat16
VMEM = pl.BlockSpec(memory_space=pltpu.VMEM)


def dot(a, b, ca, cb):
    return lax.dot_general(a, b, (((ca,), (cb,)), ((), ())), preferred_element_type=F32)


def place_kernel(n_ep, n_tp, cap, wide, x_ref, dy_ref, routes_ref, weight_ref, place_ref, *out_refs):
    toks, width = x_ref.shape
    block = width // n_tp
    me, mine = lax.axis_index("ep"), lax.axis_index("tp")
    names = lax.broadcasted_iota(jnp.int32, (n_ep, toks), 0)
    chosen = jnp.zeros((n_ep, toks), F32)
    gain = jnp.zeros((n_ep, toks), F32)
    for k in range(routes_ref.shape[0]):
        hit = routes_ref[k : k + 1, :] == names
        chosen = chosen + jnp.where(hit, 1.0, 0.0)
        gain = gain + jnp.where(hit, weight_ref[k : k + 1, :], 0.0)
    row = lax.broadcasted_iota(jnp.int32, (toks, toks), 0)
    col = lax.broadcasted_iota(jnp.int32, (toks, toks), 1)
    earlier = jnp.where(row < col, 1.0, 0.0).astype(BF16)
    rank = dot(chosen.astype(BF16), earlier, 1, 0)
    slot = lax.broadcasted_iota(jnp.int32, (cap, toks), 0).astype(F32)
    scales = []
    for d in range(n_ep):
        hit = (rank[d : d + 1, :] == slot) & (chosen[d : d + 1, :] > 0.5)
        place_ref[d] = jnp.where(hit, 1.0, 0.0).astype(BF16)
        scales.append(jnp.sum(jnp.where(hit, gain[d : d + 1, :], 0.0), axis=1, keepdims=True))

    def scale_of(target):
        out = scales[0]
        for d in range(1, n_ep):
            out = jnp.where(target == d, scales[d], out)
        return out

    def pack(target, r):
        columns = pl.ds(pl.multiple_of((mine ^ r) * block, block), block)
        pick = place_ref[target]
        rows_x = dot(pick, x_ref[:, columns], 1, 0).astype(BF16)
        rows_dy = (dot(pick, dy_ref[:, columns], 1, 0) * scale_of(target)).astype(BF16)
        return rows_x, rows_dy

    for q in list(range(2, n_ep)) + [1, 0]:
        out_ref = out_refs[q]
        for i, r in enumerate(sent_blocks(q, n_tp, wide)):
            rows_x, rows_dy = pack(me ^ q, r)
            out_ref[i, :, :block] = rows_x
            out_ref[i, :, block:] = rows_dy


def sent_blocks(q, n_tp, wide):
    return range(n_tp) if q < 2 else [0] + (wide if q // 2 == 1 else [])


def expert_kernel(n_tp, plan, cap, *refs):
    n_in = 1 + max(i for pieces in plan for i, _ in pieces)
    g_refs = refs[:n_in]
    wg_ref, wu_ref, wd_ref, dg_ref, du_ref, act_ref = refs[n_in : n_in + 6]
    tok_refs = refs[n_in + 6 :]
    block = wg_ref.shape[0] // n_tp
    mine = lax.axis_index("tp")
    offs = [pl.ds(pl.multiple_of((mine ^ r) * block, block), block) for r in range(n_tp)]
    gate = up = back = None
    for r in range(n_tp):
        rows = gather_rows(g_refs, plan[r])
        x, dy = rows[:, :block], rows[:, block:]
        g = dot(x, wg_ref[offs[r], :], 1, 0)
        u = dot(x, wu_ref[offs[r], :], 1, 0)
        b = dot(dy, wd_ref[:, offs[r]], 1, 1)
        gate, up, back = (g, u, b) if r == 0 else (gate + g, up + u, back + b)
    sig = 1.0 / (1.0 + jnp.exp(-gate))
    silu = gate * sig
    act_full = silu * up
    act_ref[...] = act_full.astype(BF16)
    d_gate = (back * up * sig * (1.0 + gate * (1.0 - sig))).astype(BF16)
    d_up = (back * silu).astype(BF16)
    dg_ref[...] = d_gate
    du_ref[...] = d_up
    n_rows = d_gate.shape[0]
    for r in range(1, n_tp):
        tok = dot(d_gate, wg_ref[offs[r], :], 1, 1) + dot(d_up, wu_ref[offs[r], :], 1, 1)
        tok_refs[r][:n_rows, :] = tok.astype(BF16)
    tok = dot(d_gate, wg_ref[offs[0], :], 1, 1) + dot(d_up, wu_ref[offs[0], :], 1, 1)
    tok_refs[0][:n_rows, :] = tok.astype(BF16)
    product = act_full * back
    high = product.astype(BF16)
    low = (product - high.astype(F32)).astype(BF16)
    ones = jnp.ones((16, product.shape[1]), BF16)
    for r in range(n_tp):
        tok_refs[r][n_rows:, :] = jnp.zeros((16, block), BF16)
    for h in range(n_rows // cap):
        span = slice(h * cap, (h + 1) * cap)
        line = (dot(ones, high[span], 1, 1) + dot(ones, low[span], 1, 1)).astype(BF16)
        for r in range(n_tp):
            tok_refs[r][n_rows:, h * 128 : h * 128 + cap] = line


def gather_rows(refs, pieces):
    parts = [refs[i][k] for i, k in pieces]
    return parts[0] if len(parts) == 1 else jnp.concatenate(parts, axis=0)


def expert_call(inputs, plan, cap, wg, wu, wd):
    n_tp = len(plan)
    rows = sum(inputs[i].shape[1] for i, _ in plan[0])
    width, hidden = wg.shape
    return pl.pallas_call(
        functools.partial(expert_kernel, n_tp, plan, cap),
        out_shape=(
            *[jax.ShapeDtypeStruct((rows, hidden), BF16)] * 3,
            *[jax.ShapeDtypeStruct((rows + 16, width // n_tp), BF16)] * n_tp,
        ),
        in_specs=[VMEM] * (len(inputs) + 3),
        out_specs=(VMEM,) * (3 + n_tp),
        cost_estimate=pl.CostEstimate(
            flops=10 * rows * width * hidden,
            bytes_accessed=6 * width * hidden + 6 * rows * width,
            transcendentals=rows * hidden,
        ),
        name="expert",
    )(*inputs, wg, wu, wd)


def merge_kernel(cap, n_in, *refs):
    rows = refs[0].shape[0] - 16
    lanes = refs[0].shape[1] // 128
    for h, out_ref in enumerate(refs[n_in:]):
        for c in range(lanes):
            total = None
            for ref in refs[:n_in]:
                term = ref[h * cap : (h + 1) * cap, c * 128 : (c + 1) * 128].astype(F32)
                total = term if total is None else total + term
            out_ref[c * cap : (c + 1) * cap, :] = total.astype(BF16)
        total = None
        for ref in refs[:n_in]:
            term = ref[rows:, h * 128 : (h + 1) * 128].astype(F32)
            total = term if total is None else total + term
        out_ref[lanes * cap :, :] = total.astype(BF16)


def merge_call(parts, cap):
    rows = parts[0].shape[0] - 16
    lanes = parts[0].shape[1] // 128
    n_out = rows // cap
    return pl.pallas_call(
        functools.partial(merge_kernel, cap, len(parts)),
        out_shape=(jax.ShapeDtypeStruct((lanes * cap + 16, 128), BF16),) * n_out,
        in_specs=[VMEM] * len(parts),
        out_specs=(VMEM,) * n_out,
        cost_estimate=pl.CostEstimate(
            flops=rows * lanes * 512, bytes_accessed=10 * rows * lanes * 128, transcendentals=0
        ),
        name="merge",
    )(*parts)


def weight_kernel(n_tp, plan, n_hidden, pos_ref, *refs):
    n_in = 1 + max(i for pieces in plan for i, _ in pieces)
    g_refs, h_refs = refs[:n_in], refs[n_in : n_in + 3 * n_hidden]
    gg_ref, gu_ref, gd_ref = refs[n_in + 3 * n_hidden :]
    block = gg_ref.shape[1]
    for r in range(n_tp):

        @pl.when(pl.program_id(0) == r)
        def _():
            rows = gather_rows(g_refs, plan[r])
            d_gate, d_up, act = (
                jnp.concatenate([h_refs[3 * i + k][...] for i in range(n_hidden)], axis=0) for k in range(3)
            )
            x, dy = rows[:, :block], rows[:, block:]
            gg_ref[0] = dot(x, d_gate, 0, 0)
            gu_ref[0] = dot(x, d_up, 0, 0)
            gd_ref[0] = dot(act, dy, 0, 0)


def weight_call(inputs, plan, hiddens, width):
    n_tp = len(plan)
    rows = sum(h[0].shape[0] for h in hiddens)
    hidden = hiddens[0][0].shape[1]
    block = width // n_tp
    position = lax.axis_index("tp").astype(jnp.int32).reshape(1)
    return pl.pallas_call(
        functools.partial(weight_kernel, n_tp, plan, len(hiddens)),
        out_shape=(
            jax.ShapeDtypeStruct((1, width, hidden), F32),
            jax.ShapeDtypeStruct((1, width, hidden), F32),
            jax.ShapeDtypeStruct((1, hidden, width), F32),
        ),
        grid_spec=pltpu.PrefetchScalarGridSpec(
            num_scalar_prefetch=1,
            grid=(n_tp,),
            in_specs=[VMEM] * (len(inputs) + 3 * len(hiddens)),
            out_specs=(
                pl.BlockSpec((1, block, hidden), lambda i, pos: (0, pos[0] ^ i, 0)),
                pl.BlockSpec((1, block, hidden), lambda i, pos: (0, pos[0] ^ i, 0)),
                pl.BlockSpec((1, hidden, block), lambda i, pos: (0, 0, pos[0] ^ i)),
            ),
        ),
        cost_estimate=pl.CostEstimate(
            flops=6 * rows * width * hidden, bytes_accessed=12 * width * hidden + 4 * rows * width, transcendentals=0
        ),
        name="weights",
    )(position, *inputs, *[h for hs in hiddens for h in hs])


def collect_kernel(n_ep, place_ref, routes_ref, weight_ref, *refs):
    back_refs, (tok_ref, rw_ref) = refs[:n_ep], refs[n_ep:]
    me = lax.axis_index("ep")
    cap = place_ref.shape[1]
    lanes = tok_ref.shape[1] // 128
    ids = routes_ref[...]
    totals = [None] * lanes
    grads = jnp.zeros(ids.shape, F32)
    for q in range(n_ep):
        pick = place_ref[me ^ q]
        for c in range(lanes):
            rows = dot(pick, back_refs[q][c * cap : (c + 1) * cap, :], 0, 0)
            totals[c] = rows if q == 0 else totals[c] + rows
        line = back_refs[q][lanes * cap :, :cap]
        value = dot(line, pick, 1, 0)[: ids.shape[0], :]
        grads = grads + jnp.where(ids == (me ^ q), value, 0.0)
    for c in range(lanes):
        tok_ref[:, c * 128 : (c + 1) * 128] = totals[c].astype(BF16)
    rw_ref[...] = grads / weight_ref[...]


def aligned(tokens, cotangent, routes, route_weight, w_gate, w_up, w_down):
    toks, width = tokens.shape
    n_ep, n_tp = lax.axis_size("ep"), lax.axis_size("tp")
    cap = 2 * toks * routes.shape[1] // n_ep
    block = width // n_tp
    wide = [n_tp - 1] if n_tp > 2 else []
    wg, wu, wd = w_gate[0], w_up[0], w_down[0]
    routes_t, weight_t = routes.T, route_weight.T
    place, *packed = pl.pallas_call(
        functools.partial(place_kernel, n_ep, n_tp, cap, wide),
        out_shape=(
            jax.ShapeDtypeStruct((n_ep, cap, toks), BF16),
            *[
                jax.ShapeDtypeStruct((len(sent_blocks(q, n_tp, wide)), cap, 2 * block), BF16)
                for q in range(n_ep)
            ],
        ),
        in_specs=[VMEM] * 4,
        out_specs=(VMEM,) * (1 + n_ep),
        name="place",
    )(tokens, cotangent, routes_t, weight_t)

    def over(axis, size, value, q):
        return lax.ppermute(value, axis, [(i, i ^ q) for i in range(size)])

    got = [packed[0]] + [over("ep", n_ep, packed[q], q) for q in range(1, n_ep)]
    inputs, plan = [], [[] for _ in range(n_tp)]

    def add(value, uses):
        for r, k in uses:
            plan[r].append((len(inputs), k))
        inputs.append(value)

    cuts = []
    for pair in range(n_ep // 2):
        messages = got[2 * pair], got[2 * pair + 1]
        if pair == 0:
            for m in messages:
                add(m, [(r, r) for r in range(n_tp)])
        else:
            sent = sent_blocks(2 * pair, n_tp, wide)
            main = jnp.concatenate([messages[0][:1], messages[1][:1]], axis=1)
            add(main, [(0, 0)])
            for m in messages if len(sent) > 1 else ():
                add(m, [(r, k) for k, r in enumerate(sent) if k])
            for r in range(1, n_tp):
                if r not in sent:
                    add(over("tp", n_tp, main, r), [(r, 0)])
        cuts.append((len(inputs), [len(p) for p in plan]))
    groups = [cuts[min(1, len(cuts) - 1)]] + ([cuts[-1]] if len(cuts) > 2 else [])
    back, hiddens = [], []
    start, begun = 0, [0] * n_tp
    for end, counts in groups:
        sub = [[(i - start, k) for i, k in plan[r][begun[r] : counts[r]]] for r in range(n_tp)]
        d_gate, d_up, act, *tok = expert_call(inputs[start:end], sub, cap, wg, wu, wd)
        hiddens.append((d_gate, d_up, act))
        moved = [tok[0]] + [over("tp", n_tp, tok[r], r) for r in range(1, n_tp)]
        for rows in merge_call(moved, cap):
            q = len(back)
            back.append(over("ep", n_ep, rows, q) if q else rows)
        start, begun = end, counts
    grad_gate, grad_up, grad_down = weight_call(inputs, plan, hiddens, width)
    grad_tokens, grad_route_weight = pl.pallas_call(
        functools.partial(collect_kernel, n_ep),
        out_shape=(
            jax.ShapeDtypeStruct((toks, block), BF16),
            jax.ShapeDtypeStruct(routes_t.shape, F32),
        ),
        in_specs=[VMEM] * (3 + n_ep),
        out_specs=(VMEM, VMEM),
        name="collect",
    )(place, routes_t, weight_t, *back)
    return grad_tokens, grad_route_weight.T, grad_gate, grad_up, grad_down


def slot_index(block_routes, experts, capacity):
    flat_ids = block_routes.reshape(-1)
    onehot = (flat_ids[:, None] == jnp.arange(experts, dtype=jnp.int32)[None, :]).astype(jnp.int32)
    earlier = jnp.cumsum(onehot, axis=0) - onehot
    return flat_ids * capacity + jnp.sum(earlier * onehot, axis=1)


def general(tokens, cotangent, routes, route_weight, w_gate, w_up, w_down):
    f32 = jnp.float32
    tok_rows, model_width = tokens.shape
    choices_row = routes.shape[1]
    experts = lax.axis_size("ep")
    capacity = 2 * tok_rows * choices_row // experts
    recv_rows = experts * capacity
    slot_ids = slot_index(routes, experts, capacity)

    def exchange(value):
        return lax.all_to_all(value, "ep", split_axis=0, concat_axis=0, tiled=True)

    send_w = jnp.zeros((recv_rows,), f32).at[slot_ids].set(route_weight.reshape(-1))
    empty = jnp.zeros((recv_rows, model_width), jnp.bfloat16)
    send_x = empty.at[slot_ids].set(jnp.repeat(tokens, choices_row, axis=0))
    send_dy = empty.at[slot_ids].set(jnp.repeat(cotangent, choices_row, axis=0))
    rows_x = exchange(send_x.reshape(experts, capacity, model_width)).reshape(recv_rows, model_width)
    rows_dy = exchange(send_dy.reshape(experts, capacity, model_width)).reshape(recv_rows, model_width)
    rows_w = exchange(send_w.reshape(experts, capacity, 1).astype(jnp.bfloat16)).astype(f32).reshape(recv_rows)
    gate_w = w_gate[0]
    up_w = w_up[0]
    down_w = w_down[0]
    gate_pre = jnp.dot(rows_x, gate_w, preferred_element_type=f32)
    up_pre = jnp.dot(rows_x, up_w, preferred_element_type=f32)
    gate_sig = jax.nn.sigmoid(gate_pre)
    act_full = gate_pre * gate_sig * up_pre
    act = act_full.astype(jnp.bfloat16)
    back_hidden = jnp.einsum("rd,fd->rf", rows_dy, down_w, preferred_element_type=f32)
    weighted_cot = (rows_w[:, None] * rows_dy.astype(f32)).astype(jnp.bfloat16)
    d_hidden = rows_w[:, None] * back_hidden
    d_gate = (d_hidden * up_pre * gate_sig * (1.0 + gate_pre * (1.0 - gate_sig))).astype(jnp.bfloat16)
    d_up = (d_hidden * gate_pre * gate_sig).astype(jnp.bfloat16)
    gate_part = jnp.sum(act_full * back_hidden, axis=1)
    token_part = jnp.einsum("rf,df->rd", d_gate, gate_w, preferred_element_type=f32)
    token_part = token_part + jnp.einsum("rf,df->rd", d_up, up_w, preferred_element_type=f32)
    grad_gate = jnp.einsum("rd,rf->df", rows_x, d_gate, preferred_element_type=f32)[None]
    grad_up = jnp.einsum("rd,rf->df", rows_x, d_up, preferred_element_type=f32)[None]
    grad_down = jnp.einsum("rf,rd->fd", act, weighted_cot, preferred_element_type=f32)[None]
    shares = lax.psum_scatter(token_part.astype(jnp.bfloat16), "tp", scatter_dimension=1, tiled=True)
    gate_total = lax.psum(gate_part, "tp")
    back_x = exchange(shares.reshape(experts, capacity, -1))
    back_gate = exchange(gate_total.reshape(experts, capacity).astype(jnp.bfloat16)).astype(f32)
    picked = back_x.reshape(recv_rows, -1)[slot_ids].astype(f32).reshape(tok_rows, choices_row, -1)
    grad_route_weight = back_gate.reshape(recv_rows)[slot_ids].reshape(tok_rows, choices_row)
    grad_tokens = jnp.sum(picked, axis=1).astype(jnp.bfloat16)
    return (grad_tokens, grad_route_weight, grad_gate, grad_up, grad_down)


def on_device(tokens, cotangent, routes, route_weight, w_gate, w_up, w_down):
    n_ep, n_tp = lax.axis_size("ep"), lax.axis_size("tp")
    toks, width = tokens.shape
    cap = 2 * toks * routes.shape[1] // n_ep
    tiles = width % (128 * n_tp) == 0 and w_gate.shape[2] % 128 == 0 and cap % 16 == 0 and cap <= 128
    tiles = tiles and n_ep * 128 <= 2 * width // n_tp * 2 and routes.shape[1] <= 16
    powers = n_ep & (n_ep - 1) == 0 and n_tp & (n_tp - 1) == 0 and n_ep > 1
    path = aligned if tiles and powers else general
    return path(tokens, cotangent, routes, route_weight, w_gate, w_up, w_down)


def solution(mesh):
    return jax.shard_map(
        on_device,
        mesh=mesh,
        in_specs=(
            P("ep", None),
            P("ep", None),
            P("ep", None),
            P("ep", None),
            P("ep", None, "tp"),
            P("ep", None, "tp"),
            P("ep", "tp", None),
        ),
        out_specs=(
            P("ep", "tp"),
            P("ep", None),
            P("ep", None, "tp"),
            P("ep", None, "tp"),
            P("ep", "tp", None),
        ),
        check_vma=False,
    )
```

```python
import functools

import jax
import jax.numpy as jnp
from jax import lax
from jax.experimental import pallas as pl
from jax.experimental.pallas import tpu as pltpu
from jax.sharding import PartitionSpec as P


F32 = jnp.float32
BF16 = jnp.bfloat16
VMEM = pl.BlockSpec(memory_space=pltpu.VMEM)


def dot(a, b, ca, cb):
    return lax.dot_general(a, b, (((ca,), (cb,)), ((), ())), preferred_element_type=F32)


def grant(mib):
    return pltpu.CompilerParams(vmem_limit_bytes=mib * 2**20)


def place_kernel(n_ep, n_tp, cap, x_ref, dy_ref, routes_ref, weight_ref, place_ref, *out_refs):
    toks, width = x_ref.shape
    block = width // n_tp
    me, mine = lax.axis_index("ep"), lax.axis_index("tp")
    names = lax.broadcasted_iota(jnp.int32, (n_ep, toks), 0)
    chosen = jnp.zeros((n_ep, toks), F32)
    gain = jnp.zeros((n_ep, toks), F32)
    for k in range(routes_ref.shape[0]):
        hit = routes_ref[k : k + 1, :] == names
        chosen = chosen + jnp.where(hit, 1.0, 0.0)
        gain = gain + jnp.where(hit, weight_ref[k : k + 1, :], 0.0)
    row = lax.broadcasted_iota(jnp.int32, (toks, toks), 0)
    col = lax.broadcasted_iota(jnp.int32, (toks, toks), 1)
    earlier = jnp.where(row < col, 1.0, 0.0).astype(BF16)
    rank = dot(chosen.astype(BF16), earlier, 1, 0)
    slot = lax.broadcasted_iota(jnp.int32, (cap, toks), 0).astype(F32)
    scales = []
    for d in range(n_ep):
        hit = (rank[d : d + 1, :] == slot) & (chosen[d : d + 1, :] > 0.5)
        place_ref[d] = jnp.where(hit, 1.0, 0.0).astype(BF16)
        scales.append(jnp.sum(jnp.where(hit, gain[d : d + 1, :], 0.0), axis=1, keepdims=True))

    def scale_of(target):
        out = scales[0]
        for d in range(1, n_ep):
            out = jnp.where(target == d, scales[d], out)
        return out

    def pack(target, r):
        columns = pl.ds(pl.multiple_of((mine ^ r) * block, block), block)
        pick = place_ref[target]
        rows_x = dot(pick, x_ref[:, columns], 1, 0).astype(BF16)
        rows_dy = (dot(pick, dy_ref[:, columns], 1, 0) * scale_of(target)).astype(BF16)
        return rows_x, rows_dy

    for q in list(range(2, n_ep)) + [1, 0]:
        out_ref = out_refs[q]
        for r in range(out_ref.shape[0]):
            rows_x, rows_dy = pack(me ^ q, r)
            out_ref[r, :, :block] = rows_x
            out_ref[r, :, block:] = rows_dy


def expert_kernel(n_tp, plan, cap, by_source, *refs):
    n_in = 1 + max(i for pieces in plan for i, _ in pieces)
    g_refs = refs[:n_in]
    wg_ref, wu_ref, wd_ref, dg_ref, du_ref, act_ref = refs[n_in : n_in + 6]
    tok_refs = refs[n_in + 6 :]
    block = wg_ref.shape[0] // n_tp
    mine = lax.axis_index("tp")
    offs = [pl.ds(pl.multiple_of((mine ^ r) * block, block), block) for r in range(n_tp)]
    gate = up = back = None
    for r in range(n_tp):
        rows = gather_rows(g_refs, plan[r])
        x, dy = rows[:, :block], rows[:, block:]
        g = dot(x, wg_ref[offs[r], :], 1, 0)
        u = dot(x, wu_ref[offs[r], :], 1, 0)
        b = dot(dy, wd_ref[:, offs[r]], 1, 1)
        gate, up, back = (g, u, b) if r == 0 else (gate + g, up + u, back + b)
    sig = 1.0 / (1.0 + jnp.exp(-gate))
    silu = gate * sig
    act_full = silu * up
    act_ref[...] = act_full.astype(BF16)
    d_gate = (back * up * sig * (1.0 + gate * (1.0 - sig))).astype(BF16)
    d_up = (back * silu).astype(BF16)
    dg_ref[...] = d_gate
    du_ref[...] = d_up
    product = act_full * back
    high = product.astype(BF16)
    low = (product - high.astype(F32)).astype(BF16)
    ones = jnp.ones((16, product.shape[1]), BF16)
    n_rows = d_gate.shape[0]
    lanes = block // 128
    for r in [*range(1, n_tp), 0]:
        tok = dot(d_gate, wg_ref[offs[r], :], 1, 1) + dot(d_up, wu_ref[offs[r], :], 1, 1)
        tok = tok.astype(BF16)
        if by_source:
            for h in range(n_rows // cap):
                for c in range(lanes):
                    at = pl.multiple_of(((mine ^ r) * lanes + c) * cap, cap)
                    tok_refs[h][pl.ds(at, cap), :] = tok[h * cap : (h + 1) * cap, c * 128 : (c + 1) * 128]
        else:
            tok_refs[r][:n_rows, :] = tok
            tok_refs[r][n_rows:, :] = jnp.zeros((16, block), BF16)
    for h in range(n_rows // cap):
        span = slice(h * cap, (h + 1) * cap)
        line = (dot(ones, high[span], 1, 1) + dot(ones, low[span], 1, 1)).astype(BF16)
        if by_source:
            tok_refs[h][n_tp * lanes * cap :, :] = jnp.zeros((16, 128), BF16)
            tok_refs[h][n_tp * lanes * cap :, :cap] = line
        else:
            for r in range(n_tp):
                tok_refs[r][n_rows:, h * 128 : h * 128 + cap] = line


def gather_rows(refs, pieces):
    parts = [refs[i][k] for i, k in pieces]
    return parts[0] if len(parts) == 1 else jnp.concatenate(parts, axis=0)


def expert_call(inputs, plan, cap, by_source, wg, wu, wd):
    n_tp = len(plan)
    rows = sum(inputs[i].shape[1] for i, _ in plan[0])
    width, hidden = wg.shape
    n_out, out = n_tp, (rows + 16, width // n_tp)
    if by_source:
        n_out, out = rows // cap, (width // 128 * cap + 16, 128)
    return pl.pallas_call(
        functools.partial(expert_kernel, n_tp, plan, cap, by_source),
        out_shape=(
            *[jax.ShapeDtypeStruct((rows, hidden), BF16)] * 3,
            *[jax.ShapeDtypeStruct(out, BF16)] * n_out,
        ),
        in_specs=[VMEM] * (len(inputs) + 3),
        out_specs=(VMEM,) * (3 + n_out),
        cost_estimate=pl.CostEstimate(
            flops=10 * rows * width * hidden,
            bytes_accessed=6 * width * hidden + 6 * rows * width,
            transcendentals=rows * hidden,
        ),
        compiler_params=grant(24),
        name="expert",
    )(*inputs, wg, wu, wd)


def merge_kernel(cap, n_in, *refs):
    rows = refs[0].shape[0] - 16
    lanes = refs[0].shape[1] // 128
    for h, out_ref in enumerate(refs[n_in:]):
        for c in range(lanes):
            total = None
            for ref in refs[:n_in]:
                term = ref[h * cap : (h + 1) * cap, c * 128 : (c + 1) * 128].astype(F32)
                total = term if total is None else total + term
            out_ref[c * cap : (c + 1) * cap, :] = total.astype(BF16)
        total = None
        for ref in refs[:n_in]:
            term = ref[rows:, h * 128 : (h + 1) * 128].astype(F32)
            total = term if total is None else total + term
        out_ref[lanes * cap :, :] = total.astype(BF16)


def merge_call(parts, cap):
    rows = parts[0].shape[0] - 16
    lanes = parts[0].shape[1] // 128
    n_out = rows // cap
    return pl.pallas_call(
        functools.partial(merge_kernel, cap, len(parts)),
        out_shape=(jax.ShapeDtypeStruct((lanes * cap + 16, 128), BF16),) * n_out,
        in_specs=[VMEM] * len(parts),
        out_specs=(VMEM,) * n_out,
        cost_estimate=pl.CostEstimate(
            flops=rows * lanes * 512, bytes_accessed=10 * rows * lanes * 128, transcendentals=0
        ),
        compiler_params=grant(8),
        name="merge",
    )(*parts)


def weight_kernel(n_tp, plan, n_hidden, pos_ref, *refs):
    n_in = 1 + max(i for pieces in plan for i, _ in pieces)
    g_refs, h_refs = refs[:n_in], refs[n_in : n_in + 3 * n_hidden]
    gg_ref, gu_ref, gd_ref = refs[n_in + 3 * n_hidden :]
    block = gg_ref.shape[1]
    for r in range(n_tp):

        @pl.when(pl.program_id(0) == r)
        def _():
            rows = gather_rows(g_refs, plan[r])
            d_gate, d_up, act = (
                jnp.concatenate([h_refs[3 * i + k][...] for i in range(n_hidden)], axis=0) for k in range(3)
            )
            x, dy = rows[:, :block], rows[:, block:]
            gg_ref[0] = dot(x, d_gate, 0, 0)
            gu_ref[0] = dot(x, d_up, 0, 0)
            gd_ref[0] = dot(act, dy, 0, 0)


def weight_call(inputs, plan, hiddens, width):
    n_tp = len(plan)
    rows = sum(h[0].shape[0] for h in hiddens)
    hidden = hiddens[0][0].shape[1]
    block = width // n_tp
    position = lax.axis_index("tp").astype(jnp.int32).reshape(1)
    return pl.pallas_call(
        functools.partial(weight_kernel, n_tp, plan, len(hiddens)),
        out_shape=(
            jax.ShapeDtypeStruct((1, width, hidden), F32),
            jax.ShapeDtypeStruct((1, width, hidden), F32),
            jax.ShapeDtypeStruct((1, hidden, width), F32),
        ),
        grid_spec=pltpu.PrefetchScalarGridSpec(
            num_scalar_prefetch=1,
            grid=(n_tp,),
            in_specs=[VMEM] * (len(inputs) + 3 * len(hiddens)),
            out_specs=(
                pl.BlockSpec((1, block, hidden), lambda i, pos: (0, pos[0] ^ i, 0)),
                pl.BlockSpec((1, block, hidden), lambda i, pos: (0, pos[0] ^ i, 0)),
                pl.BlockSpec((1, hidden, block), lambda i, pos: (0, 0, pos[0] ^ i)),
            ),
        ),
        cost_estimate=pl.CostEstimate(
            flops=6 * rows * width * hidden, bytes_accessed=12 * width * hidden + 4 * rows * width, transcendentals=0
        ),
        name="weights",
    )(position, *inputs, *[h for hs in hiddens for h in hs])


def near_kernel(n_tp, n_near, place_ref, routes_ref, *refs):
    rows_refs, out_refs = refs[:n_near], refs[n_near:]
    me, mine = lax.axis_index("ep"), lax.axis_index("tp")
    cap, toks = place_ref.shape[1:]
    lanes = out_refs[0].shape[1] // 128
    ids = routes_ref[...]
    grads = jnp.zeros(ids.shape, F32)
    for q in range(n_near):
        line = rows_refs[q][n_tp * lanes * cap :, :cap]
        value = dot(line, place_ref[me ^ q], 1, 0)[: ids.shape[0], :]
        grads = grads + jnp.where(ids == (me ^ q), value, 0.0)
    for r in range(n_tp):
        for c in range(lanes):
            at = pl.multiple_of(((mine ^ r) * lanes + c) * cap, cap)
            total = None
            for q in range(n_near):
                rows = dot(place_ref[me ^ q], rows_refs[q][pl.ds(at, cap), :], 0, 0)
                total = rows if q == 0 else total + rows
            out_refs[r][:toks, c * 128 : (c + 1) * 128] = total.astype(BF16)
        out_refs[r][toks:, :] = jnp.zeros((16, lanes * 128), BF16)
        out_refs[r][toks : toks + ids.shape[0], :toks] = grads.astype(BF16)


def near_call(place, routes_t, rows, n_tp, block):
    toks = routes_t.shape[1]
    return pl.pallas_call(
        functools.partial(near_kernel, n_tp, len(rows)),
        out_shape=(jax.ShapeDtypeStruct((toks + 16, block), BF16),) * n_tp,
        in_specs=[VMEM] * (2 + len(rows)),
        out_specs=(VMEM,) * n_tp,
        cost_estimate=pl.CostEstimate(
            flops=2 * toks * place.shape[1] * len(rows) * n_tp * block,
            bytes_accessed=6 * toks * n_tp * block,
            transcendentals=0,
        ),
        compiler_params=grant(16),
        name="near",
    )(place, routes_t, *rows)


def collect_kernel(n_ep, n_near, n_tp, place_ref, routes_ref, weight_ref, *refs):
    near_refs, far_refs = refs[:n_tp], refs[n_tp : n_tp + n_ep - n_near]
    tok_ref, rw_ref = refs[n_tp + n_ep - n_near :]
    me = lax.axis_index("ep")
    cap, toks = place_ref.shape[1:]
    lanes = tok_ref.shape[1] // 128
    ids = routes_ref[...]
    grads = jnp.zeros(ids.shape, F32)
    for near_ref in near_refs:
        grads = grads + near_ref[toks : toks + 16, :toks].astype(F32)[: ids.shape[0], :]
    totals = []
    for c in range(lanes):
        total = None
        for near_ref in near_refs:
            term = near_ref[:toks, c * 128 : (c + 1) * 128].astype(F32)
            total = term if total is None else total + term
        totals.append(total)
    for q in range(n_near, n_ep):
        pick = place_ref[me ^ q]
        far_ref = far_refs[q - n_near]
        for c in range(lanes):
            totals[c] = totals[c] + dot(pick, far_ref[c * cap : (c + 1) * cap, :], 0, 0)
        line = far_ref[lanes * cap :, :cap]
        value = dot(line, pick, 1, 0)[: ids.shape[0], :]
        grads = grads + jnp.where(ids == (me ^ q), value, 0.0)
    for c in range(lanes):
        tok_ref[:, c * 128 : (c + 1) * 128] = totals[c].astype(BF16)
    rw_ref[...] = grads / weight_ref[...]


def aligned(tokens, cotangent, routes, route_weight, w_gate, w_up, w_down):
    toks, width = tokens.shape
    n_ep, n_tp = lax.axis_size("ep"), lax.axis_size("tp")
    cap = 2 * toks * routes.shape[1] // n_ep
    block = width // n_tp
    wg, wu, wd = w_gate[0], w_up[0], w_down[0]
    routes_t, weight_t = routes.T, route_weight.T
    place, *packed = pl.pallas_call(
        functools.partial(place_kernel, n_ep, n_tp, cap),
        out_shape=(
            jax.ShapeDtypeStruct((n_ep, cap, toks), BF16),
            *[jax.ShapeDtypeStruct((n_tp if q < 2 else 1, cap, 2 * block), BF16) for q in range(n_ep)],
        ),
        in_specs=[VMEM] * 4,
        out_specs=(VMEM,) * (1 + n_ep),
        name="place",
    )(tokens, cotangent, routes_t, weight_t)

    def over(axis, size, value, q):
        return lax.ppermute(value, axis, [(i, i ^ q) for i in range(size)])

    got = [packed[0]] + [over("ep", n_ep, packed[q], q) for q in range(1, n_ep)]
    inputs, plan = [], [[] for _ in range(n_tp)]

    def add(value, uses):
        for r, k in uses:
            plan[r].append((len(inputs), k))
        inputs.append(value)

    cuts = []
    for pair in range(n_ep // 2):
        messages = got[2 * pair], got[2 * pair + 1]
        if pair == 0:
            for m in messages:
                add(m, [(r, r) for r in range(n_tp)])
        else:
            main = jnp.concatenate(messages, axis=1)
            add(main, [(0, 0)])
            for r in range(1, n_tp):
                add(over("tp", n_tp, main, r), [(r, 0)])
        cuts.append((len(inputs), [len(p) for p in plan]))
    n_near = min(4, n_ep)
    far, hiddens = [], []
    start, begun = 0, [0] * n_tp
    for number, (end, counts) in enumerate(cuts[n_near // 2 - 1 :]):
        sub = [[(i - start, k) for i, k in plan[r][begun[r] : counts[r]]] for r in range(n_tp)]
        d_gate, d_up, act, *tok = expert_call(inputs[start:end], sub, cap, number == 0, wg, wu, wd)
        hiddens.append((d_gate, d_up, act))
        if number == 0:
            rows = [tok[0]] + [over("ep", n_ep, tok[q], q) for q in range(1, n_near)]
            tok = near_call(place, routes_t, rows, n_tp, block)
        moved = [tok[0]] + [over("tp", n_tp, tok[r], r) for r in range(1, n_tp)]
        if number == 0:
            near = moved
        else:
            merged = merge_call(moved, cap)
            for rows in merged:
                far.append(over("ep", n_ep, rows, n_near + len(far)))
        start, begun = end, counts
    grad_gate, grad_up, grad_down = weight_call(inputs, plan, hiddens, width)
    grad_tokens, grad_route_weight = pl.pallas_call(
        functools.partial(collect_kernel, n_ep, n_near, n_tp),
        out_shape=(
            jax.ShapeDtypeStruct((toks, block), BF16),
            jax.ShapeDtypeStruct(routes_t.shape, F32),
        ),
        in_specs=[VMEM] * (3 + n_tp + n_ep - n_near),
        out_specs=(VMEM, VMEM),
        compiler_params=grant(16),
        name="collect",
    )(place, routes_t, weight_t, *near, *far)
    return grad_tokens, grad_route_weight.T, grad_gate, grad_up, grad_down


def slot_index(block_routes, experts, capacity):
    flat_ids = block_routes.reshape(-1)
    onehot = (flat_ids[:, None] == jnp.arange(experts, dtype=jnp.int32)[None, :]).astype(jnp.int32)
    earlier = jnp.cumsum(onehot, axis=0) - onehot
    return flat_ids * capacity + jnp.sum(earlier * onehot, axis=1)


def general(tokens, cotangent, routes, route_weight, w_gate, w_up, w_down):
    f32 = jnp.float32
    tok_rows, model_width = tokens.shape
    choices_row = routes.shape[1]
    experts = lax.axis_size("ep")
    capacity = 2 * tok_rows * choices_row // experts
    recv_rows = experts * capacity
    slot_ids = slot_index(routes, experts, capacity)

    def exchange(value):
        return lax.all_to_all(value, "ep", split_axis=0, concat_axis=0, tiled=True)

    send_w = jnp.zeros((recv_rows,), f32).at[slot_ids].set(route_weight.reshape(-1))
    empty = jnp.zeros((recv_rows, model_width), jnp.bfloat16)
    send_x = empty.at[slot_ids].set(jnp.repeat(tokens, choices_row, axis=0))
    send_dy = empty.at[slot_ids].set(jnp.repeat(cotangent, choices_row, axis=0))
    rows_x = exchange(send_x.reshape(experts, capacity, model_width)).reshape(recv_rows, model_width)
    rows_dy = exchange(send_dy.reshape(experts, capacity, model_width)).reshape(recv_rows, model_width)
    rows_w = exchange(send_w.reshape(experts, capacity, 1).astype(jnp.bfloat16)).astype(f32).reshape(recv_rows)
    gate_w = w_gate[0]
    up_w = w_up[0]
    down_w = w_down[0]
    gate_pre = jnp.dot(rows_x, gate_w, preferred_element_type=f32)
    up_pre = jnp.dot(rows_x, up_w, preferred_element_type=f32)
    gate_sig = jax.nn.sigmoid(gate_pre)
    act_full = gate_pre * gate_sig * up_pre
    act = act_full.astype(jnp.bfloat16)
    back_hidden = jnp.einsum("rd,fd->rf", rows_dy, down_w, preferred_element_type=f32)
    weighted_cot = (rows_w[:, None] * rows_dy.astype(f32)).astype(jnp.bfloat16)
    d_hidden = rows_w[:, None] * back_hidden
    d_gate = (d_hidden * up_pre * gate_sig * (1.0 + gate_pre * (1.0 - gate_sig))).astype(jnp.bfloat16)
    d_up = (d_hidden * gate_pre * gate_sig).astype(jnp.bfloat16)
    gate_part = jnp.sum(act_full * back_hidden, axis=1)
    token_part = jnp.einsum("rf,df->rd", d_gate, gate_w, preferred_element_type=f32)
    token_part = token_part + jnp.einsum("rf,df->rd", d_up, up_w, preferred_element_type=f32)
    grad_gate = jnp.einsum("rd,rf->df", rows_x, d_gate, preferred_element_type=f32)[None]
    grad_up = jnp.einsum("rd,rf->df", rows_x, d_up, preferred_element_type=f32)[None]
    grad_down = jnp.einsum("rf,rd->fd", act, weighted_cot, preferred_element_type=f32)[None]
    shares = lax.psum_scatter(token_part.astype(jnp.bfloat16), "tp", scatter_dimension=1, tiled=True)
    gate_total = lax.psum(gate_part, "tp")
    back_x = exchange(shares.reshape(experts, capacity, -1))
    back_gate = exchange(gate_total.reshape(experts, capacity).astype(jnp.bfloat16)).astype(f32)
    picked = back_x.reshape(recv_rows, -1)[slot_ids].astype(f32).reshape(tok_rows, choices_row, -1)
    grad_route_weight = back_gate.reshape(recv_rows)[slot_ids].reshape(tok_rows, choices_row)
    grad_tokens = jnp.sum(picked, axis=1).astype(jnp.bfloat16)
    return (grad_tokens, grad_route_weight, grad_gate, grad_up, grad_down)


def on_device(tokens, cotangent, routes, route_weight, w_gate, w_up, w_down):
    n_ep, n_tp = lax.axis_size("ep"), lax.axis_size("tp")
    toks, width = tokens.shape
    cap = 2 * toks * routes.shape[1] // n_ep
    tiles = width % (128 * n_tp) == 0 and w_gate.shape[2] % 128 == 0 and cap % 16 == 0 and cap <= 128
    tiles = tiles and n_ep * 128 <= 2 * width // n_tp * 2 and routes.shape[1] <= 16
    powers = n_ep & (n_ep - 1) == 0 and n_tp & (n_tp - 1) == 0 and n_ep > 1
    path = aligned if tiles and powers else general
    return path(tokens, cotangent, routes, route_weight, w_gate, w_up, w_down)


def solution(mesh):
    return jax.shard_map(
        on_device,
        mesh=mesh,
        in_specs=(
            P("ep", None),
            P("ep", None),
            P("ep", None),
            P("ep", None),
            P("ep", None, "tp"),
            P("ep", None, "tp"),
            P("ep", "tp", None),
        ),
        out_specs=(
            P("ep", "tp"),
            P("ep", None),
            P("ep", None, "tp"),
            P("ep", None, "tp"),
            P("ep", "tp", None),
        ),
        check_vma=False,
    )
```

```python
import functools

import jax
import jax.numpy as jnp
from jax import lax
from jax.experimental import pallas as pl
from jax.experimental.pallas import tpu as pltpu
from jax.sharding import PartitionSpec as P


F32 = jnp.float32
BF16 = jnp.bfloat16
VMEM = pl.BlockSpec(memory_space=pltpu.VMEM)
HBM = pl.BlockSpec(memory_space=pltpu.HBM)


def dot(a, b, ca, cb):
    return lax.dot_general(a, b, (((ca,), (cb,)), ((), ())), preferred_element_type=F32)


def grant(mib):
    return pltpu.CompilerParams(vmem_limit_bytes=mib * 2**20)


def place_kernel(n_ep, cap, x_hbm, dy_hbm, routes_ref, weight_ref, place_ref, scale_ref, *rest):
    out_refs, (x_ref, dy_ref, sems) = rest[: n_ep - 2], rest[n_ep - 2 :]
    toks, block = x_ref.shape
    me, mine = lax.axis_index("ep"), lax.axis_index("tp")
    columns = pl.ds(pl.multiple_of(mine * block, block), block)
    copies = [
        pltpu.make_async_copy(x_hbm.at[:, columns], x_ref, sems.at[0]),
        pltpu.make_async_copy(dy_hbm.at[:, columns], dy_ref, sems.at[1]),
    ]
    for copy in copies:
        copy.start()
    names = lax.broadcasted_iota(jnp.int32, (n_ep, toks), 0)
    chosen = jnp.zeros((n_ep, toks), F32)
    gain = jnp.zeros((n_ep, toks), F32)
    for k in range(routes_ref.shape[0]):
        hit = routes_ref[k : k + 1, :] == names
        chosen = chosen + jnp.where(hit, 1.0, 0.0)
        gain = gain + jnp.where(hit, weight_ref[k : k + 1, :], 0.0)
    row = lax.broadcasted_iota(jnp.int32, (toks, toks), 0)
    col = lax.broadcasted_iota(jnp.int32, (toks, toks), 1)
    earlier = jnp.where(row < col, 1.0, 0.0).astype(BF16)
    rank = dot(chosen.astype(BF16), earlier, 1, 0)
    slot = lax.broadcasted_iota(jnp.int32, (cap, toks), 0).astype(F32)
    for d in range(n_ep):
        hit = (rank[d : d + 1, :] == slot) & (chosen[d : d + 1, :] > 0.5)
        place_ref[d] = jnp.where(hit, 1.0, 0.0).astype(BF16)
        scale = jnp.sum(jnp.where(hit, gain[d : d + 1, :], 0.0), axis=1, keepdims=True)
        scale_ref[d] = jnp.broadcast_to(scale, (cap, 128))
    for copy in copies:
        copy.wait()
    for q in range(2, n_ep):
        pack(place_ref, scale_ref, me ^ q, x_ref[...], dy_ref[...], out_refs[q - 2], 0)


def pack(place_ref, scale_ref, target, x, dy, out_ref, r):
    block = x.shape[1]
    pick = place_ref[target]
    out_ref[r, :, :block] = dot(pick, x, 1, 0).astype(BF16)
    out_ref[r, :, block:] = (dot(pick, dy, 1, 0) * scale_ref[target][:, :1]).astype(BF16)


def beside_kernel(n_tp, place_ref, scale_ref, x_hbm, dy_hbm, partner_ref, own_ref, *rest):
    last_refs, (x_ref, dy_ref, sems) = rest[:-3], rest[-3:]
    block = x_hbm.shape[1] // n_tp
    me, mine = lax.axis_index("ep"), lax.axis_index("tp")
    copies = []
    for r in range(n_tp):
        columns = pl.ds(pl.multiple_of((mine ^ r) * block, block), block)
        copies.append(pltpu.make_async_copy(x_hbm.at[:, columns], x_ref.at[r], sems.at[0, r]))
        copies.append(pltpu.make_async_copy(dy_hbm.at[:, columns], dy_ref.at[r], sems.at[1, r]))
    for copy in copies:
        copy.start()
    for r in range(n_tp):
        copies[2 * r].wait()
        copies[2 * r + 1].wait()
        for q, out_ref in ((1, partner_ref), (0, own_ref)):
            pack(place_ref, scale_ref, me ^ q, x_ref[r], dy_ref[r], out_ref, r)
    for q, out_ref in enumerate(last_refs):
        pack(place_ref, scale_ref, me ^ (2 + q), x_ref[n_tp - 1], dy_ref[n_tp - 1], out_ref, 0)


def expert_kernel(n_tp, plan, cap, by_source, *refs):
    n_in = 1 + max(i for pieces in plan for i, _ in pieces)
    g_refs = refs[:n_in]
    wg_ref, wu_ref, wd_ref, hidden_ref = refs[n_in : n_in + 4]
    tok_refs = refs[n_in + 4 :]
    hidden = wg_ref.shape[1]
    block = wg_ref.shape[0] // n_tp
    mine = lax.axis_index("tp")
    offs = [pl.ds(pl.multiple_of((mine ^ r) * block, block), block) for r in range(n_tp)]
    gate = up = back = None
    for r in range(n_tp):
        rows = gather_rows(g_refs, plan[r])
        x, dy = rows[:, :block], rows[:, block:]
        g = dot(x, wg_ref[offs[r], :], 1, 0)
        u = dot(x, wu_ref[offs[r], :], 1, 0)
        b = dot(dy, wd_ref[:, offs[r]], 1, 1)
        gate, up, back = (g, u, b) if r == 0 else (gate + g, up + u, back + b)
    sig = 1.0 / (1.0 + jnp.exp(-gate))
    silu = gate * sig
    act_full = silu * up
    hidden_ref[:, 2 * hidden :] = act_full.astype(BF16)
    d_gate = (back * up * sig * (1.0 + gate * (1.0 - sig))).astype(BF16)
    d_up = (back * silu).astype(BF16)
    hidden_ref[:, :hidden] = d_gate
    hidden_ref[:, hidden : 2 * hidden] = d_up
    product = act_full * back
    high = product.astype(BF16)
    low = (product - high.astype(F32)).astype(BF16)
    ones = jnp.ones((16, product.shape[1]), BF16)
    n_rows = d_gate.shape[0]
    lanes = block // 128
    for r in [*range(1, n_tp), 0]:
        tok = dot(d_gate, wg_ref[offs[r], :], 1, 1) + dot(d_up, wu_ref[offs[r], :], 1, 1)
        tok = tok.astype(BF16)
        if by_source:
            for h in range(n_rows // cap):
                for c in range(lanes):
                    at = pl.multiple_of(((mine ^ r) * lanes + c) * cap, cap)
                    tok_refs[h][pl.ds(at, cap), :] = tok[h * cap : (h + 1) * cap, c * 128 : (c + 1) * 128]
        else:
            tok_refs[r][:n_rows, :] = tok
            tok_refs[r][n_rows:, :] = jnp.zeros((16, block), BF16)
    for h in range(n_rows // cap):
        span = slice(h * cap, (h + 1) * cap)
        line = (dot(ones, high[span], 1, 1) + dot(ones, low[span], 1, 1)).astype(BF16)
        if by_source:
            tok_refs[h][n_tp * lanes * cap :, :] = jnp.zeros((16, 128), BF16)
            tok_refs[h][n_tp * lanes * cap :, :cap] = line
        else:
            for r in range(n_tp):
                tok_refs[r][n_rows:, h * 128 : h * 128 + cap] = line


def gather_rows(refs, pieces):
    parts = [refs[i][k] for i, k in pieces]
    return parts[0] if len(parts) == 1 else jnp.concatenate(parts, axis=0)


def expert_call(inputs, plan, cap, by_source, wg, wu, wd):
    n_tp = len(plan)
    rows = sum(inputs[i].shape[1] for i, _ in plan[0])
    width, hidden = wg.shape
    n_out, out = n_tp, (rows + 16, width // n_tp)
    if by_source:
        n_out, out = rows // cap, (width // 128 * cap + 16, 128)
    return pl.pallas_call(
        functools.partial(expert_kernel, n_tp, plan, cap, by_source),
        out_shape=(
            jax.ShapeDtypeStruct((rows, 3 * hidden), BF16),
            *[jax.ShapeDtypeStruct(out, BF16)] * n_out,
        ),
        in_specs=[VMEM] * (len(inputs) + 3),
        out_specs=(VMEM,) * (1 + n_out),
        cost_estimate=pl.CostEstimate(
            flops=10 * rows * width * hidden,
            bytes_accessed=6 * width * hidden + 6 * rows * width,
            transcendentals=rows * hidden,
        ),
        compiler_params=grant(24),
        name="expert",
    )(*inputs, wg, wu, wd)


def merge_kernel(cap, n_in, *refs):
    rows = refs[0].shape[0] - 16
    lanes = refs[0].shape[1] // 128
    for h, out_ref in enumerate(refs[n_in:]):
        for c in range(lanes):
            total = None
            for ref in refs[:n_in]:
                term = ref[h * cap : (h + 1) * cap, c * 128 : (c + 1) * 128].astype(F32)
                total = term if total is None else total + term
            out_ref[c * cap : (c + 1) * cap, :] = total.astype(BF16)
        total = None
        for ref in refs[:n_in]:
            term = ref[rows:, h * 128 : (h + 1) * 128].astype(F32)
            total = term if total is None else total + term
        out_ref[lanes * cap :, :] = total.astype(BF16)


def merge_call(parts, cap):
    rows = parts[0].shape[0] - 16
    lanes = parts[0].shape[1] // 128
    n_out = rows // cap
    return pl.pallas_call(
        functools.partial(merge_kernel, cap, len(parts)),
        out_shape=(jax.ShapeDtypeStruct((lanes * cap + 16, 128), BF16),) * n_out,
        in_specs=[VMEM] * len(parts),
        out_specs=(VMEM,) * n_out,
        cost_estimate=pl.CostEstimate(
            flops=rows * lanes * 512, bytes_accessed=10 * rows * lanes * 128, transcendentals=0
        ),
        compiler_params=grant(8),
        name="merge",
    )(*parts)


def weight_kernel(n_tp, plan, n_hidden, pos_ref, *refs):
    n_in = 1 + max(i for pieces in plan for i, _ in pieces)
    g_refs, h_refs = refs[:n_in], refs[n_in : n_in + n_hidden]
    gg_ref, gu_ref, gd_ref = refs[n_in + n_hidden :]
    _, block, hidden = gg_ref.shape
    for r in range(n_tp):

        @pl.when(pl.program_id(0) == r)
        def _():
            rows = gather_rows(g_refs, plan[r])
            d_gate, d_up, act = (
                jnp.concatenate([ref[:, k * hidden : (k + 1) * hidden] for ref in h_refs], axis=0) for k in range(3)
            )
            x, dy = rows[:, :block], rows[:, block:]
            gg_ref[0] = dot(x, d_gate, 0, 0)
            gu_ref[0] = dot(x, d_up, 0, 0)
            gd_ref[0] = dot(act, dy, 0, 0)


def weight_call(inputs, plan, hiddens, width):
    n_tp = len(plan)
    rows = sum(h.shape[0] for h in hiddens)
    hidden = hiddens[0].shape[1] // 3
    block = width // n_tp
    position = lax.axis_index("tp").astype(jnp.int32).reshape(1)
    return pl.pallas_call(
        functools.partial(weight_kernel, n_tp, plan, len(hiddens)),
        out_shape=(
            jax.ShapeDtypeStruct((1, width, hidden), F32),
            jax.ShapeDtypeStruct((1, width, hidden), F32),
            jax.ShapeDtypeStruct((1, hidden, width), F32),
        ),
        grid_spec=pltpu.PrefetchScalarGridSpec(
            num_scalar_prefetch=1,
            grid=(n_tp,),
            in_specs=[VMEM] * (len(inputs) + len(hiddens)),
            out_specs=(
                pl.BlockSpec((1, block, hidden), lambda i, pos: (0, pos[0] ^ i, 0)),
                pl.BlockSpec((1, block, hidden), lambda i, pos: (0, pos[0] ^ i, 0)),
                pl.BlockSpec((1, hidden, block), lambda i, pos: (0, 0, pos[0] ^ i)),
            ),
        ),
        cost_estimate=pl.CostEstimate(
            flops=6 * rows * width * hidden, bytes_accessed=12 * width * hidden + 4 * rows * width, transcendentals=0
        ),
        name="weights",
    )(position, *inputs, *hiddens)


def near_kernel(n_tp, n_near, place_ref, routes_ref, *refs):
    rows_refs, out_refs = refs[:n_near], refs[n_near:]
    me, mine = lax.axis_index("ep"), lax.axis_index("tp")
    cap, toks = place_ref.shape[1:]
    lanes = out_refs[0].shape[1] // 128
    ids = routes_ref[...]
    grads = jnp.zeros(ids.shape, F32)
    for q in range(n_near):
        line = rows_refs[q][n_tp * lanes * cap :, :cap]
        value = dot(line, place_ref[me ^ q], 1, 0)[: ids.shape[0], :]
        grads = grads + jnp.where(ids == (me ^ q), value, 0.0)
    for r in range(n_tp):
        for c in range(lanes):
            at = pl.multiple_of(((mine ^ r) * lanes + c) * cap, cap)
            total = None
            for q in range(n_near):
                rows = dot(place_ref[me ^ q], rows_refs[q][pl.ds(at, cap), :], 0, 0)
                total = rows if q == 0 else total + rows
            out_refs[r][:toks, c * 128 : (c + 1) * 128] = total.astype(BF16)
        out_refs[r][toks:, :] = jnp.zeros((16, lanes * 128), BF16)
        out_refs[r][toks : toks + ids.shape[0], :toks] = grads.astype(BF16)


def near_call(place, routes_t, rows, n_tp, block):
    toks = routes_t.shape[1]
    return pl.pallas_call(
        functools.partial(near_kernel, n_tp, len(rows)),
        out_shape=(jax.ShapeDtypeStruct((toks + 16, block), BF16),) * n_tp,
        in_specs=[VMEM] * (2 + len(rows)),
        out_specs=(VMEM,) * n_tp,
        cost_estimate=pl.CostEstimate(
            flops=2 * toks * place.shape[1] * len(rows) * n_tp * block,
            bytes_accessed=6 * toks * n_tp * block,
            transcendentals=0,
        ),
        compiler_params=grant(16),
        name="near",
    )(place, routes_t, *rows)


def collect_kernel(n_ep, n_near, n_tp, place_ref, routes_ref, weight_ref, *refs):
    near_refs, far_refs = refs[:n_tp], refs[n_tp : n_tp + n_ep - n_near]
    tok_ref, rw_ref = refs[n_tp + n_ep - n_near :]
    me = lax.axis_index("ep")
    cap, toks = place_ref.shape[1:]
    lanes = tok_ref.shape[1] // 128
    ids = routes_ref[...]
    grads = jnp.zeros(ids.shape, F32)
    for near_ref in near_refs:
        grads = grads + near_ref[toks : toks + 16, :toks].astype(F32)[: ids.shape[0], :]
    totals = []
    for c in range(lanes):
        total = None
        for near_ref in near_refs:
            term = near_ref[:toks, c * 128 : (c + 1) * 128].astype(F32)
            total = term if total is None else total + term
        totals.append(total)
    for q in range(n_near, n_ep):
        pick = place_ref[me ^ q]
        far_ref = far_refs[q - n_near]
        for c in range(lanes):
            totals[c] = totals[c] + dot(pick, far_ref[c * cap : (c + 1) * cap, :], 0, 0)
        line = far_ref[lanes * cap :, :cap]
        value = dot(line, pick, 1, 0)[: ids.shape[0], :]
        grads = grads + jnp.where(ids == (me ^ q), value, 0.0)
    for c in range(lanes):
        tok_ref[:, c * 128 : (c + 1) * 128] = totals[c].astype(BF16)
    rw_ref[...] = grads / weight_ref[...]


def aligned(tokens, cotangent, routes, route_weight, w_gate, w_up, w_down):
    toks, width = tokens.shape
    n_ep, n_tp = lax.axis_size("ep"), lax.axis_size("tp")
    cap = 2 * toks * routes.shape[1] // n_ep
    block = width // n_tp
    wg, wu, wd = w_gate[0], w_up[0], w_down[0]
    routes_t, weight_t = routes.T, route_weight.T
    message = jax.ShapeDtypeStruct((1, cap, 2 * block), BF16)
    near_message = jax.ShapeDtypeStruct((n_tp, cap, 2 * block), BF16)
    place, scale, *packed = pl.pallas_call(
        functools.partial(place_kernel, n_ep, cap),
        out_shape=(
            jax.ShapeDtypeStruct((n_ep, cap, toks), BF16),
            jax.ShapeDtypeStruct((n_ep, cap, 128), F32),
            *[message] * (n_ep - 2),
        ),
        in_specs=[HBM, HBM, VMEM, VMEM],
        out_specs=(VMEM,) * n_ep,
        scratch_shapes=[
            pltpu.VMEM((toks, block), BF16),
            pltpu.VMEM((toks, block), BF16),
            pltpu.SemaphoreType.DMA((2,)),
        ],
        compiler_params=grant(53),
        name="place",
    )(tokens, cotangent, routes_t, weight_t)
    n_last = 2 if n_tp > 2 and n_ep > 2 else 0
    partner, own, *last = pl.pallas_call(
        functools.partial(beside_kernel, n_tp),
        out_shape=(near_message, near_message, *[message] * n_last),
        in_specs=[VMEM, VMEM, HBM, HBM],
        out_specs=(VMEM,) * (2 + n_last),
        scratch_shapes=[
            pltpu.VMEM((n_tp, toks, block), BF16),
            pltpu.VMEM((n_tp, toks, block), BF16),
            pltpu.SemaphoreType.DMA((2, n_tp)),
        ],
        cost_estimate=pl.CostEstimate(flops=8 * cap * toks * width, bytes_accessed=8 * toks * width, transcendentals=0),
        compiler_params=grant(16),
        name="beside",
    )(place, scale, tokens, cotangent)
    packed = [own, partner, *packed]

    def over(axis, size, value, q):
        return lax.ppermute(value, axis, [(i, i ^ q) for i in range(size)])

    got = [packed[0]] + [over("ep", n_ep, packed[q], q) for q in range(1, n_ep)]
    inputs, plan = [], [[] for _ in range(n_tp)]

    def add(value, uses):
        for r, k in uses:
            plan[r].append((len(inputs), k))
        inputs.append(value)

    cuts = []
    for pair in range(n_ep // 2):
        messages = got[2 * pair], got[2 * pair + 1]
        if pair == 0:
            for m in messages:
                add(m, [(r, r) for r in range(n_tp)])
        else:
            main = jnp.concatenate(messages, axis=1)
            add(main, [(0, 0)])
            direct = n_tp - 1 if pair == 1 and last else n_tp
            for r in range(1, direct):
                add(over("tp", n_tp, main, r), [(r, 0)])
            for q, rows in enumerate(last if direct < n_tp else []):
                add(over("ep", n_ep, rows, 2 + q), [(n_tp - 1, 0)])
        cuts.append((len(inputs), [len(p) for p in plan]))
    n_near = min(4, n_ep)
    far, hiddens = [], []
    start, begun = 0, [0] * n_tp
    for number, (end, counts) in enumerate(cuts[n_near // 2 - 1 :]):
        sub = [[(i - start, k) for i, k in plan[r][begun[r] : counts[r]]] for r in range(n_tp)]
        kept, *tok = expert_call(inputs[start:end], sub, cap, number == 0, wg, wu, wd)
        hiddens.append(kept)
        if number == 0:
            rows = [tok[0]] + [over("ep", n_ep, tok[q], q) for q in range(1, n_near)]
            tok = near_call(place, routes_t, rows, n_tp, block)
        moved = [tok[0]] + [over("tp", n_tp, tok[r], r) for r in range(1, n_tp)]
        if number == 0:
            near = moved
        else:
            merged = merge_call(moved, cap)
            for rows in merged:
                far.append(over("ep", n_ep, rows, n_near + len(far)))
        start, begun = end, counts
    grad_gate, grad_up, grad_down = weight_call(inputs, plan, hiddens, width)
    grad_tokens, grad_route_weight = pl.pallas_call(
        functools.partial(collect_kernel, n_ep, n_near, n_tp),
        out_shape=(
            jax.ShapeDtypeStruct((toks, block), BF16),
            jax.ShapeDtypeStruct(routes_t.shape, F32),
        ),
        in_specs=[VMEM] * (3 + n_tp + n_ep - n_near),
        out_specs=(VMEM, VMEM),
        compiler_params=grant(16),
        name="collect",
    )(place, routes_t, weight_t, *near, *far)
    return grad_tokens, grad_route_weight.T, grad_gate, grad_up, grad_down


def slot_index(block_routes, experts, capacity):
    flat_ids = block_routes.reshape(-1)
    onehot = (flat_ids[:, None] == jnp.arange(experts, dtype=jnp.int32)[None, :]).astype(jnp.int32)
    earlier = jnp.cumsum(onehot, axis=0) - onehot
    return flat_ids * capacity + jnp.sum(earlier * onehot, axis=1)


def general(tokens, cotangent, routes, route_weight, w_gate, w_up, w_down):
    f32 = jnp.float32
    tok_rows, model_width = tokens.shape
    choices_row = routes.shape[1]
    experts = lax.axis_size("ep")
    capacity = 2 * tok_rows * choices_row // experts
    recv_rows = experts * capacity
    slot_ids = slot_index(routes, experts, capacity)

    def exchange(value):
        return lax.all_to_all(value, "ep", split_axis=0, concat_axis=0, tiled=True)

    send_w = jnp.zeros((recv_rows,), f32).at[slot_ids].set(route_weight.reshape(-1))
    empty = jnp.zeros((recv_rows, model_width), jnp.bfloat16)
    send_x = empty.at[slot_ids].set(jnp.repeat(tokens, choices_row, axis=0))
    send_dy = empty.at[slot_ids].set(jnp.repeat(cotangent, choices_row, axis=0))
    rows_x = exchange(send_x.reshape(experts, capacity, model_width)).reshape(recv_rows, model_width)
    rows_dy = exchange(send_dy.reshape(experts, capacity, model_width)).reshape(recv_rows, model_width)
    rows_w = exchange(send_w.reshape(experts, capacity, 1).astype(jnp.bfloat16)).astype(f32).reshape(recv_rows)
    gate_w = w_gate[0]
    up_w = w_up[0]
    down_w = w_down[0]
    gate_pre = jnp.dot(rows_x, gate_w, preferred_element_type=f32)
    up_pre = jnp.dot(rows_x, up_w, preferred_element_type=f32)
    gate_sig = jax.nn.sigmoid(gate_pre)
    act_full = gate_pre * gate_sig * up_pre
    act = act_full.astype(jnp.bfloat16)
    back_hidden = jnp.einsum("rd,fd->rf", rows_dy, down_w, preferred_element_type=f32)
    weighted_cot = (rows_w[:, None] * rows_dy.astype(f32)).astype(jnp.bfloat16)
    d_hidden = rows_w[:, None] * back_hidden
    d_gate = (d_hidden * up_pre * gate_sig * (1.0 + gate_pre * (1.0 - gate_sig))).astype(jnp.bfloat16)
    d_up = (d_hidden * gate_pre * gate_sig).astype(jnp.bfloat16)
    gate_part = jnp.sum(act_full * back_hidden, axis=1)
    token_part = jnp.einsum("rf,df->rd", d_gate, gate_w, preferred_element_type=f32)
    token_part = token_part + jnp.einsum("rf,df->rd", d_up, up_w, preferred_element_type=f32)
    grad_gate = jnp.einsum("rd,rf->df", rows_x, d_gate, preferred_element_type=f32)[None]
    grad_up = jnp.einsum("rd,rf->df", rows_x, d_up, preferred_element_type=f32)[None]
    grad_down = jnp.einsum("rf,rd->fd", act, weighted_cot, preferred_element_type=f32)[None]
    shares = lax.psum_scatter(token_part.astype(jnp.bfloat16), "tp", scatter_dimension=1, tiled=True)
    gate_total = lax.psum(gate_part, "tp")
    back_x = exchange(shares.reshape(experts, capacity, -1))
    back_gate = exchange(gate_total.reshape(experts, capacity).astype(jnp.bfloat16)).astype(f32)
    picked = back_x.reshape(recv_rows, -1)[slot_ids].astype(f32).reshape(tok_rows, choices_row, -1)
    grad_route_weight = back_gate.reshape(recv_rows)[slot_ids].reshape(tok_rows, choices_row)
    grad_tokens = jnp.sum(picked, axis=1).astype(jnp.bfloat16)
    return (grad_tokens, grad_route_weight, grad_gate, grad_up, grad_down)


def on_device(tokens, cotangent, routes, route_weight, w_gate, w_up, w_down):
    n_ep, n_tp = lax.axis_size("ep"), lax.axis_size("tp")
    toks, width = tokens.shape
    cap = 2 * toks * routes.shape[1] // n_ep
    tiles = width % (128 * n_tp) == 0 and w_gate.shape[2] % 128 == 0 and cap % 16 == 0 and cap <= 128
    tiles = tiles and n_ep * 128 <= 2 * width // n_tp * 2 and routes.shape[1] <= 16
    powers = n_ep & (n_ep - 1) == 0 and n_tp & (n_tp - 1) == 0 and n_ep > 1
    path = aligned if tiles and powers else general
    return path(tokens, cotangent, routes, route_weight, w_gate, w_up, w_down)


def solution(mesh):
    return jax.shard_map(
        on_device,
        mesh=mesh,
        in_specs=(
            P("ep", None),
            P("ep", None),
            P("ep", None),
            P("ep", None),
            P("ep", None, "tp"),
            P("ep", None, "tp"),
            P("ep", "tp", None),
        ),
        out_specs=(
            P("ep", "tp"),
            P("ep", None),
            P("ep", None, "tp"),
            P("ep", None, "tp"),
            P("ep", "tp", None),
        ),
        check_vma=False,
    )
```

```python
import functools

import jax
import jax.numpy as jnp
from jax import lax
from jax.experimental import pallas as pl
from jax.experimental.pallas import tpu as pltpu
from jax.sharding import PartitionSpec as P


F32 = jnp.float32
BF16 = jnp.bfloat16
VMEM = pl.BlockSpec(memory_space=pltpu.VMEM)
HBM = pl.BlockSpec(memory_space=pltpu.HBM)


def dot(a, b, ca, cb):
    return lax.dot_general(a, b, (((ca,), (cb,)), ((), ())), preferred_element_type=F32)


def grant(mib):
    return pltpu.CompilerParams(vmem_limit_bytes=mib * 2**20)


def place_kernel(n_ep, n_tp, cap, x_hbm, dy_hbm, routes_ref, weight_ref, place_ref, scale_ref, *rest):
    out_refs, (x_ref, dy_ref, sems) = rest[:-3], rest[-3:]
    n_blocks, toks, block = x_ref.shape
    me, mine = lax.axis_index("ep"), lax.axis_index("tp")
    copies = []
    for i, r in enumerate((0, n_tp - 1)[:n_blocks]):
        columns = pl.ds(pl.multiple_of((mine ^ r) * block, block), block)
        copies.append(pltpu.make_async_copy(x_hbm.at[:, columns], x_ref.at[i], sems.at[0, i]))
        copies.append(pltpu.make_async_copy(dy_hbm.at[:, columns], dy_ref.at[i], sems.at[1, i]))
    for copy in copies:
        copy.start()
    names = lax.broadcasted_iota(jnp.int32, (n_ep, toks), 0)
    chosen = jnp.zeros((n_ep, toks), F32)
    gain = jnp.zeros((n_ep, toks), F32)
    for k in range(routes_ref.shape[0]):
        hit = routes_ref[k : k + 1, :] == names
        chosen = chosen + jnp.where(hit, 1.0, 0.0)
        gain = gain + jnp.where(hit, weight_ref[k : k + 1, :], 0.0)
    row = lax.broadcasted_iota(jnp.int32, (toks, toks), 0)
    col = lax.broadcasted_iota(jnp.int32, (toks, toks), 1)
    earlier = jnp.where(row < col, 1.0, 0.0).astype(BF16)
    rank = dot(chosen.astype(BF16), earlier, 1, 0)
    slot = lax.broadcasted_iota(jnp.int32, (cap, toks), 0).astype(F32)
    for d in range(n_ep):
        hit = (rank[d : d + 1, :] == slot) & (chosen[d : d + 1, :] > 0.5)
        place_ref[d] = jnp.where(hit, 1.0, 0.0).astype(BF16)
        scale = jnp.sum(jnp.where(hit, gain[d : d + 1, :], 0.0), axis=1, keepdims=True)
        scale_ref[d] = jnp.broadcast_to(scale, (cap, 128))
    for copy in copies:
        copy.wait()
    for q in range(2, n_ep):
        pack(place_ref, scale_ref, me ^ q, x_ref[0], dy_ref[0], out_refs[q - 2], 0)
    for q, out_ref in enumerate(out_refs[n_ep - 2 :]):
        pack(place_ref, scale_ref, me ^ (2 + q), x_ref[1], dy_ref[1], out_ref, 0)


def pack(place_ref, scale_ref, target, x, dy, out_ref, r):
    block = x.shape[1]
    pick = place_ref[target]
    out_ref[r, :, :block] = dot(pick, x, 1, 0).astype(BF16)
    out_ref[r, :, block:] = (dot(pick, dy, 1, 0) * scale_ref[target][:, :1]).astype(BF16)


def beside_kernel(n_tp, place_ref, scale_ref, x_hbm, dy_hbm, partner_ref, own_ref, x_ref, dy_ref, sems):
    block = x_hbm.shape[1] // n_tp
    me, mine = lax.axis_index("ep"), lax.axis_index("tp")
    copies = []
    for r in range(n_tp):
        columns = pl.ds(pl.multiple_of((mine ^ r) * block, block), block)
        copies.append(pltpu.make_async_copy(x_hbm.at[:, columns], x_ref.at[r], sems.at[0, r]))
        copies.append(pltpu.make_async_copy(dy_hbm.at[:, columns], dy_ref.at[r], sems.at[1, r]))
    for copy in copies:
        copy.start()
    for r in range(n_tp):
        copies[2 * r].wait()
        copies[2 * r + 1].wait()
        for q, out_ref in ((1, partner_ref), (0, own_ref)):
            pack(place_ref, scale_ref, me ^ q, x_ref[r], dy_ref[r], out_ref, r)


def expert_kernel(n_tp, plan, cap, by_source, *refs):
    n_in = 1 + max(i for pieces in plan for i, _ in pieces)
    g_refs = refs[:n_in]
    wg_ref, wu_ref, wd_ref, hidden_ref = refs[n_in : n_in + 4]
    tok_refs = refs[n_in + 4 :]
    hidden = wg_ref.shape[1]
    block = wg_ref.shape[0] // n_tp
    mine = lax.axis_index("tp")
    offs = [pl.ds(pl.multiple_of((mine ^ r) * block, block), block) for r in range(n_tp)]
    gate = up = back = None
    for r in range(n_tp):
        rows = gather_rows(g_refs, plan[r])
        x, dy = rows[:, :block], rows[:, block:]
        g = dot(x, wg_ref[offs[r], :], 1, 0)
        u = dot(x, wu_ref[offs[r], :], 1, 0)
        b = dot(dy, wd_ref[:, offs[r]], 1, 1)
        gate, up, back = (g, u, b) if r == 0 else (gate + g, up + u, back + b)
    sig = 1.0 / (1.0 + jnp.exp(-gate))
    silu = gate * sig
    act_full = silu * up
    hidden_ref[:, 2 * hidden :] = act_full.astype(BF16)
    d_gate = (back * up * sig * (1.0 + gate * (1.0 - sig))).astype(BF16)
    d_up = (back * silu).astype(BF16)
    hidden_ref[:, :hidden] = d_gate
    hidden_ref[:, hidden : 2 * hidden] = d_up
    product = act_full * back
    high = product.astype(BF16)
    low = (product - high.astype(F32)).astype(BF16)
    ones = jnp.ones((16, product.shape[1]), BF16)
    n_rows = d_gate.shape[0]
    lanes = block // 128
    for r in [*range(1, n_tp), 0]:
        tok = dot(d_gate, wg_ref[offs[r], :], 1, 1) + dot(d_up, wu_ref[offs[r], :], 1, 1)
        tok = tok.astype(BF16)
        if by_source:
            for h in range(n_rows // cap):
                for c in range(lanes):
                    at = pl.multiple_of(((mine ^ r) * lanes + c) * cap, cap)
                    tok_refs[h][pl.ds(at, cap), :] = tok[h * cap : (h + 1) * cap, c * 128 : (c + 1) * 128]
        else:
            tok_refs[r][:n_rows, :] = tok
            tok_refs[r][n_rows:, :] = jnp.zeros((16, block), BF16)
    for h in range(n_rows // cap):
        span = slice(h * cap, (h + 1) * cap)
        line = (dot(ones, high[span], 1, 1) + dot(ones, low[span], 1, 1)).astype(BF16)
        if by_source:
            tok_refs[h][n_tp * lanes * cap :, :] = jnp.zeros((16, 128), BF16)
            tok_refs[h][n_tp * lanes * cap :, :cap] = line
        else:
            for r in range(n_tp):
                tok_refs[r][n_rows:, h * 128 : h * 128 + cap] = line


def gather_rows(refs, pieces):
    parts = [refs[i][k] for i, k in pieces]
    return parts[0] if len(parts) == 1 else jnp.concatenate(parts, axis=0)


def expert_call(inputs, plan, cap, by_source, wg, wu, wd):
    n_tp = len(plan)
    rows = sum(inputs[i].shape[1] for i, _ in plan[0])
    width, hidden = wg.shape
    n_out, out = n_tp, (rows + 16, width // n_tp)
    if by_source:
        n_out, out = rows // cap, (width // 128 * cap + 16, 128)
    return pl.pallas_call(
        functools.partial(expert_kernel, n_tp, plan, cap, by_source),
        out_shape=(
            jax.ShapeDtypeStruct((rows, 3 * hidden), BF16),
            *[jax.ShapeDtypeStruct(out, BF16)] * n_out,
        ),
        in_specs=[VMEM] * (len(inputs) + 3),
        out_specs=(VMEM,) * (1 + n_out),
        cost_estimate=pl.CostEstimate(
            flops=10 * rows * width * hidden,
            bytes_accessed=6 * width * hidden + 6 * rows * width,
            transcendentals=rows * hidden,
        ),
        compiler_params=grant(24),
        name="expert",
    )(*inputs, wg, wu, wd)


def merge_kernel(cap, n_in, *refs):
    rows = refs[0].shape[0] - 16
    lanes = refs[0].shape[1] // 128
    for h, out_ref in enumerate(refs[n_in:]):
        for c in range(lanes):
            total = None
            for ref in refs[:n_in]:
                term = ref[h * cap : (h + 1) * cap, c * 128 : (c + 1) * 128].astype(F32)
                total = term if total is None else total + term
            out_ref[c * cap : (c + 1) * cap, :] = total.astype(BF16)
        total = None
        for ref in refs[:n_in]:
            term = ref[rows:, h * 128 : (h + 1) * 128].astype(F32)
            total = term if total is None else total + term
        out_ref[lanes * cap :, :] = total.astype(BF16)


def merge_call(parts, cap):
    rows = parts[0].shape[0] - 16
    lanes = parts[0].shape[1] // 128
    n_out = rows // cap
    return pl.pallas_call(
        functools.partial(merge_kernel, cap, len(parts)),
        out_shape=(jax.ShapeDtypeStruct((lanes * cap + 16, 128), BF16),) * n_out,
        in_specs=[VMEM] * len(parts),
        out_specs=(VMEM,) * n_out,
        cost_estimate=pl.CostEstimate(
            flops=rows * lanes * 512, bytes_accessed=10 * rows * lanes * 128, transcendentals=0
        ),
        compiler_params=grant(8),
        name="merge",
    )(*parts)


def weight_kernel(n_tp, plan, n_hidden, pos_ref, *refs):
    n_in = 1 + max(i for pieces in plan for i, _ in pieces)
    g_refs, h_refs = refs[:n_in], refs[n_in : n_in + n_hidden]
    gg_ref, gu_ref, gd_ref = refs[n_in + n_hidden :]
    _, block, hidden = gg_ref.shape
    for r in range(n_tp):

        @pl.when(pl.program_id(0) == r)
        def _():
            rows = gather_rows(g_refs, plan[r])
            d_gate, d_up, act = (
                jnp.concatenate([ref[:, k * hidden : (k + 1) * hidden] for ref in h_refs], axis=0) for k in range(3)
            )
            x, dy = rows[:, :block], rows[:, block:]
            gg_ref[0] = dot(x, d_gate, 0, 0)
            gu_ref[0] = dot(x, d_up, 0, 0)
            gd_ref[0] = dot(act, dy, 0, 0)


def weight_call(inputs, plan, hiddens, width):
    n_tp = len(plan)
    rows = sum(h.shape[0] for h in hiddens)
    hidden = hiddens[0].shape[1] // 3
    block = width // n_tp
    position = lax.axis_index("tp").astype(jnp.int32).reshape(1)
    return pl.pallas_call(
        functools.partial(weight_kernel, n_tp, plan, len(hiddens)),
        out_shape=(
            jax.ShapeDtypeStruct((1, width, hidden), F32),
            jax.ShapeDtypeStruct((1, width, hidden), F32),
            jax.ShapeDtypeStruct((1, hidden, width), F32),
        ),
        grid_spec=pltpu.PrefetchScalarGridSpec(
            num_scalar_prefetch=1,
            grid=(n_tp,),
            in_specs=[VMEM] * (len(inputs) + len(hiddens)),
            out_specs=(
                pl.BlockSpec((1, block, hidden), lambda i, pos: (0, pos[0] ^ i, 0)),
                pl.BlockSpec((1, block, hidden), lambda i, pos: (0, pos[0] ^ i, 0)),
                pl.BlockSpec((1, hidden, block), lambda i, pos: (0, 0, pos[0] ^ i)),
            ),
        ),
        cost_estimate=pl.CostEstimate(
            flops=6 * rows * width * hidden, bytes_accessed=12 * width * hidden + 4 * rows * width, transcendentals=0
        ),
        name="weights",
    )(position, *inputs, *hiddens)


def near_kernel(n_tp, n_near, place_ref, routes_ref, *refs):
    rows_refs, out_refs = refs[:n_near], refs[n_near:]
    me, mine = lax.axis_index("ep"), lax.axis_index("tp")
    cap, toks = place_ref.shape[1:]
    lanes = out_refs[0].shape[1] // 128
    ids = routes_ref[...]
    grads = jnp.zeros(ids.shape, F32)
    for q in range(n_near):
        line = rows_refs[q][n_tp * lanes * cap :, :cap]
        value = dot(line, place_ref[me ^ q], 1, 0)[: ids.shape[0], :]
        grads = grads + jnp.where(ids == (me ^ q), value, 0.0)
    for r in range(n_tp):
        for c in range(lanes):
            at = pl.multiple_of(((mine ^ r) * lanes + c) * cap, cap)
            total = None
            for q in range(n_near):
                rows = dot(place_ref[me ^ q], rows_refs[q][pl.ds(at, cap), :], 0, 0)
                total = rows if q == 0 else total + rows
            out_refs[r][:toks, c * 128 : (c + 1) * 128] = total.astype(BF16)
        out_refs[r][toks:, :] = jnp.zeros((16, lanes * 128), BF16)
        out_refs[r][toks : toks + ids.shape[0], :toks] = grads.astype(BF16)


def near_call(place, routes_t, rows, n_tp, block):
    toks = routes_t.shape[1]
    return pl.pallas_call(
        functools.partial(near_kernel, n_tp, len(rows)),
        out_shape=(jax.ShapeDtypeStruct((toks + 16, block), BF16),) * n_tp,
        in_specs=[VMEM] * (2 + len(rows)),
        out_specs=(VMEM,) * n_tp,
        cost_estimate=pl.CostEstimate(
            flops=2 * toks * place.shape[1] * len(rows) * n_tp * block,
            bytes_accessed=6 * toks * n_tp * block,
            transcendentals=0,
        ),
        compiler_params=grant(16),
        name="near",
    )(place, routes_t, *rows)


def collect_kernel(n_ep, n_near, n_tp, place_ref, routes_ref, weight_ref, *refs):
    near_refs, far_refs = refs[:n_tp], refs[n_tp : n_tp + n_ep - n_near]
    tok_ref, rw_ref = refs[n_tp + n_ep - n_near :]
    me = lax.axis_index("ep")
    cap, toks = place_ref.shape[1:]
    lanes = tok_ref.shape[1] // 128
    ids = routes_ref[...]
    grads = jnp.zeros(ids.shape, F32)
    for near_ref in near_refs:
        grads = grads + near_ref[toks : toks + 16, :toks].astype(F32)[: ids.shape[0], :]
    totals = []
    for c in range(lanes):
        total = None
        for near_ref in near_refs:
            term = near_ref[:toks, c * 128 : (c + 1) * 128].astype(F32)
            total = term if total is None else total + term
        totals.append(total)
    for q in range(n_near, n_ep):
        pick = place_ref[me ^ q]
        far_ref = far_refs[q - n_near]
        for c in range(lanes):
            totals[c] = totals[c] + dot(pick, far_ref[c * cap : (c + 1) * cap, :], 0, 0)
        line = far_ref[lanes * cap :, :cap]
        value = dot(line, pick, 1, 0)[: ids.shape[0], :]
        grads = grads + jnp.where(ids == (me ^ q), value, 0.0)
    for c in range(lanes):
        tok_ref[:, c * 128 : (c + 1) * 128] = totals[c].astype(BF16)
    rw_ref[...] = grads / weight_ref[...]


def aligned(tokens, cotangent, routes, route_weight, w_gate, w_up, w_down):
    toks, width = tokens.shape
    n_ep, n_tp = lax.axis_size("ep"), lax.axis_size("tp")
    cap = 2 * toks * routes.shape[1] // n_ep
    block = width // n_tp
    wg, wu, wd = w_gate[0], w_up[0], w_down[0]
    routes_t, weight_t = routes.T, route_weight.T
    message = jax.ShapeDtypeStruct((1, cap, 2 * block), BF16)
    near_message = jax.ShapeDtypeStruct((n_tp, cap, 2 * block), BF16)
    n_last = 2 if n_tp > 2 and n_ep > 2 else 0
    n_blocks = 2 if n_last else 1
    place, scale, *packed = pl.pallas_call(
        functools.partial(place_kernel, n_ep, n_tp, cap),
        out_shape=(
            jax.ShapeDtypeStruct((n_ep, cap, toks), BF16),
            jax.ShapeDtypeStruct((n_ep, cap, 128), F32),
            *[message] * (n_ep - 2 + n_last),
        ),
        in_specs=[HBM, HBM, VMEM, VMEM],
        out_specs=(VMEM,) * (n_ep + n_last),
        scratch_shapes=[
            pltpu.VMEM((n_blocks, toks, block), BF16),
            pltpu.VMEM((n_blocks, toks, block), BF16),
            pltpu.SemaphoreType.DMA((2, n_blocks)),
        ],
        compiler_params=grant(53),
        name="place",
    )(tokens, cotangent, routes_t, weight_t)
    partner, own = pl.pallas_call(
        functools.partial(beside_kernel, n_tp),
        out_shape=(near_message, near_message),
        in_specs=[VMEM, VMEM, HBM, HBM],
        out_specs=(VMEM, VMEM),
        scratch_shapes=[
            pltpu.VMEM((n_tp, toks, block), BF16),
            pltpu.VMEM((n_tp, toks, block), BF16),
            pltpu.SemaphoreType.DMA((2, n_tp)),
        ],
        cost_estimate=pl.CostEstimate(flops=8 * cap * toks * width, bytes_accessed=8 * toks * width, transcendentals=0),
        compiler_params=grant(16),
        name="beside",
    )(place, scale, tokens, cotangent)
    last = packed[n_ep - 2 :]
    packed = [own, partner, *packed[: n_ep - 2]]

    def over(axis, size, value, q):
        return lax.ppermute(value, axis, [(i, i ^ q) for i in range(size)])

    got = [packed[0]] + [over("ep", n_ep, packed[q], q) for q in range(1, n_ep)]
    inputs, plan = [], [[] for _ in range(n_tp)]

    def add(value, uses):
        for r, k in uses:
            plan[r].append((len(inputs), k))
        inputs.append(value)

    cuts = []
    for pair in range(n_ep // 2):
        messages = got[2 * pair], got[2 * pair + 1]
        if pair == 0:
            for m in messages:
                add(m, [(r, r) for r in range(n_tp)])
        else:
            main = jnp.concatenate(messages, axis=1)
            add(main, [(0, 0)])
            direct = n_tp - 1 if pair == 1 and last else n_tp
            for r in range(1, direct):
                add(over("tp", n_tp, main, r), [(r, 0)])
            for q, rows in enumerate(last if direct < n_tp else []):
                add(over("ep", n_ep, rows, 2 + q), [(n_tp - 1, 0)])
        cuts.append((len(inputs), [len(p) for p in plan]))
    n_near = min(4, n_ep)
    far, hiddens = [], []
    start, begun = 0, [0] * n_tp
    for number, (end, counts) in enumerate(cuts[n_near // 2 - 1 :]):
        sub = [[(i - start, k) for i, k in plan[r][begun[r] : counts[r]]] for r in range(n_tp)]
        kept, *tok = expert_call(inputs[start:end], sub, cap, number == 0, wg, wu, wd)
        hiddens.append(kept)
        if number == 0:
            rows = [tok[0]] + [over("ep", n_ep, tok[q], q) for q in range(1, n_near)]
            tok = near_call(place, routes_t, rows, n_tp, block)
        moved = [tok[0]] + [over("tp", n_tp, tok[r], r) for r in range(1, n_tp)]
        if number == 0:
            near = moved
        else:
            merged = merge_call(moved, cap)
            for rows in merged:
                far.append(over("ep", n_ep, rows, n_near + len(far)))
        start, begun = end, counts
    grad_gate, grad_up, grad_down = weight_call(inputs, plan, hiddens, width)
    grad_tokens, grad_route_weight = pl.pallas_call(
        functools.partial(collect_kernel, n_ep, n_near, n_tp),
        out_shape=(
            jax.ShapeDtypeStruct((toks, block), BF16),
            jax.ShapeDtypeStruct(routes_t.shape, F32),
        ),
        in_specs=[VMEM] * (3 + n_tp + n_ep - n_near),
        out_specs=(VMEM, VMEM),
        compiler_params=grant(16),
        name="collect",
    )(place, routes_t, weight_t, *near, *far)
    return grad_tokens, grad_route_weight.T, grad_gate, grad_up, grad_down


def slot_index(block_routes, experts, capacity):
    flat_ids = block_routes.reshape(-1)
    onehot = (flat_ids[:, None] == jnp.arange(experts, dtype=jnp.int32)[None, :]).astype(jnp.int32)
    earlier = jnp.cumsum(onehot, axis=0) - onehot
    return flat_ids * capacity + jnp.sum(earlier * onehot, axis=1)


def general(tokens, cotangent, routes, route_weight, w_gate, w_up, w_down):
    f32 = jnp.float32
    tok_rows, model_width = tokens.shape
    choices_row = routes.shape[1]
    experts = lax.axis_size("ep")
    capacity = 2 * tok_rows * choices_row // experts
    recv_rows = experts * capacity
    slot_ids = slot_index(routes, experts, capacity)

    def exchange(value):
        return lax.all_to_all(value, "ep", split_axis=0, concat_axis=0, tiled=True)

    send_w = jnp.zeros((recv_rows,), f32).at[slot_ids].set(route_weight.reshape(-1))
    empty = jnp.zeros((recv_rows, model_width), jnp.bfloat16)
    send_x = empty.at[slot_ids].set(jnp.repeat(tokens, choices_row, axis=0))
    send_dy = empty.at[slot_ids].set(jnp.repeat(cotangent, choices_row, axis=0))
    rows_x = exchange(send_x.reshape(experts, capacity, model_width)).reshape(recv_rows, model_width)
    rows_dy = exchange(send_dy.reshape(experts, capacity, model_width)).reshape(recv_rows, model_width)
    rows_w = exchange(send_w.reshape(experts, capacity, 1).astype(jnp.bfloat16)).astype(f32).reshape(recv_rows)
    gate_w = w_gate[0]
    up_w = w_up[0]
    down_w = w_down[0]
    gate_pre = jnp.dot(rows_x, gate_w, preferred_element_type=f32)
    up_pre = jnp.dot(rows_x, up_w, preferred_element_type=f32)
    gate_sig = jax.nn.sigmoid(gate_pre)
    act_full = gate_pre * gate_sig * up_pre
    act = act_full.astype(jnp.bfloat16)
    back_hidden = jnp.einsum("rd,fd->rf", rows_dy, down_w, preferred_element_type=f32)
    weighted_cot = (rows_w[:, None] * rows_dy.astype(f32)).astype(jnp.bfloat16)
    d_hidden = rows_w[:, None] * back_hidden
    d_gate = (d_hidden * up_pre * gate_sig * (1.0 + gate_pre * (1.0 - gate_sig))).astype(jnp.bfloat16)
    d_up = (d_hidden * gate_pre * gate_sig).astype(jnp.bfloat16)
    gate_part = jnp.sum(act_full * back_hidden, axis=1)
    token_part = jnp.einsum("rf,df->rd", d_gate, gate_w, preferred_element_type=f32)
    token_part = token_part + jnp.einsum("rf,df->rd", d_up, up_w, preferred_element_type=f32)
    grad_gate = jnp.einsum("rd,rf->df", rows_x, d_gate, preferred_element_type=f32)[None]
    grad_up = jnp.einsum("rd,rf->df", rows_x, d_up, preferred_element_type=f32)[None]
    grad_down = jnp.einsum("rf,rd->fd", act, weighted_cot, preferred_element_type=f32)[None]
    shares = lax.psum_scatter(token_part.astype(jnp.bfloat16), "tp", scatter_dimension=1, tiled=True)
    gate_total = lax.psum(gate_part, "tp")
    back_x = exchange(shares.reshape(experts, capacity, -1))
    back_gate = exchange(gate_total.reshape(experts, capacity).astype(jnp.bfloat16)).astype(f32)
    picked = back_x.reshape(recv_rows, -1)[slot_ids].astype(f32).reshape(tok_rows, choices_row, -1)
    grad_route_weight = back_gate.reshape(recv_rows)[slot_ids].reshape(tok_rows, choices_row)
    grad_tokens = jnp.sum(picked, axis=1).astype(jnp.bfloat16)
    return (grad_tokens, grad_route_weight, grad_gate, grad_up, grad_down)


def on_device(tokens, cotangent, routes, route_weight, w_gate, w_up, w_down):
    n_ep, n_tp = lax.axis_size("ep"), lax.axis_size("tp")
    toks, width = tokens.shape
    cap = 2 * toks * routes.shape[1] // n_ep
    tiles = width % (128 * n_tp) == 0 and w_gate.shape[2] % 128 == 0 and cap % 16 == 0 and cap <= 128
    tiles = tiles and n_ep * 128 <= 2 * width // n_tp * 2 and routes.shape[1] <= 16
    powers = n_ep & (n_ep - 1) == 0 and n_tp & (n_tp - 1) == 0 and n_ep > 1
    path = aligned if tiles and powers else general
    return path(tokens, cotangent, routes, route_weight, w_gate, w_up, w_down)


def solution(mesh):
    return jax.shard_map(
        on_device,
        mesh=mesh,
        in_specs=(
            P("ep", None),
            P("ep", None),
            P("ep", None),
            P("ep", None),
            P("ep", None, "tp"),
            P("ep", None, "tp"),
            P("ep", "tp", None),
        ),
        out_specs=(
            P("ep", "tp"),
            P("ep", None),
            P("ep", None, "tp"),
            P("ep", None, "tp"),
            P("ep", "tp", None),
        ),
        check_vma=False,
    )
```

```python
import functools

import jax
import jax.numpy as jnp
from jax import lax
from jax.experimental import pallas as pl
from jax.experimental.pallas import tpu as pltpu
from jax.sharding import PartitionSpec as P


F32 = jnp.float32
BF16 = jnp.bfloat16
VMEM = pl.BlockSpec(memory_space=pltpu.VMEM)
HBM = pl.BlockSpec(memory_space=pltpu.HBM)
NOMINAL = pl.CostEstimate(flops=1024, bytes_accessed=1024, transcendentals=0)


def dot(a, b, ca, cb):
    return lax.dot_general(a, b, (((ca,), (cb,)), ((), ())), preferred_element_type=F32)


def grant(mib):
    return pltpu.CompilerParams(vmem_limit_bytes=mib * 2**20)


def place_kernel(n_ep, n_tp, cap, lasts, x_hbm, dy_hbm, routes_ref, weight_ref, place_ref, scale_ref, *rest):
    out_refs, (x_ref, dy_ref, sems) = rest[:-3], rest[-3:]
    n_blocks, toks, block = x_ref.shape
    me, mine = lax.axis_index("ep"), lax.axis_index("tp")
    copies = []
    for i, r in enumerate((0, n_tp - 1)[:n_blocks]):
        columns = pl.ds(pl.multiple_of((mine ^ r) * block, block), block)
        copies.append(pltpu.make_async_copy(x_hbm.at[:, columns], x_ref.at[i], sems.at[0, i]))
        copies.append(pltpu.make_async_copy(dy_hbm.at[:, columns], dy_ref.at[i], sems.at[1, i]))
    for copy in copies:
        copy.start()
    names = lax.broadcasted_iota(jnp.int32, (n_ep, toks), 0)
    chosen = jnp.zeros((n_ep, toks), F32)
    gain = jnp.zeros((n_ep, toks), F32)
    for k in range(routes_ref.shape[0]):
        hit = routes_ref[k : k + 1, :] == names
        chosen = chosen + jnp.where(hit, 1.0, 0.0)
        gain = gain + jnp.where(hit, weight_ref[k : k + 1, :], 0.0)
    row = lax.broadcasted_iota(jnp.int32, (toks, toks), 0)
    col = lax.broadcasted_iota(jnp.int32, (toks, toks), 1)
    earlier = jnp.where(row < col, 1.0, 0.0).astype(BF16)
    rank = dot(chosen.astype(BF16), earlier, 1, 0)
    slot = lax.broadcasted_iota(jnp.int32, (cap, toks), 0).astype(F32)
    for d in range(n_ep):
        hit = (rank[d : d + 1, :] == slot) & (chosen[d : d + 1, :] > 0.5)
        place_ref[d] = jnp.where(hit, 1.0, 0.0).astype(BF16)
        scale = jnp.sum(jnp.where(hit, gain[d : d + 1, :], 0.0), axis=1, keepdims=True)
        scale_ref[d] = jnp.broadcast_to(scale, (cap, 128))
    for copy in copies:
        copy.wait()
    for q in range(2, n_ep):
        pack(place_ref, scale_ref, me ^ q, x_ref[0], dy_ref[0], out_refs[q - 2], 0)
    for q, out_ref in zip(lasts, out_refs[n_ep - 2 :]):
        pack(place_ref, scale_ref, me ^ q, x_ref[1], dy_ref[1], out_ref, 0)


def pack(place_ref, scale_ref, target, x, dy, out_ref, r):
    block = x.shape[1]
    pick = place_ref[target]
    out_ref[r, :, :block] = dot(pick, x, 1, 0).astype(BF16)
    out_ref[r, :, block:] = (dot(pick, dy, 1, 0) * scale_ref[target][:, :1]).astype(BF16)


def beside_kernel(n_tp, place_ref, scale_ref, x_hbm, dy_hbm, partner_ref, own_ref, x_ref, dy_ref, sems):
    block = x_hbm.shape[1] // n_tp
    me, mine = lax.axis_index("ep"), lax.axis_index("tp")
    copies = []
    for r in range(n_tp):
        columns = pl.ds(pl.multiple_of((mine ^ r) * block, block), block)
        copies.append(pltpu.make_async_copy(x_hbm.at[:, columns], x_ref.at[r], sems.at[0, r]))
        copies.append(pltpu.make_async_copy(dy_hbm.at[:, columns], dy_ref.at[r], sems.at[1, r]))
    for copy in copies:
        copy.start()
    for r in range(n_tp):
        copies[2 * r].wait()
        copies[2 * r + 1].wait()
        for q, out_ref in ((1, partner_ref), (0, own_ref)):
            pack(place_ref, scale_ref, me ^ q, x_ref[r], dy_ref[r], out_ref, r)


def expert_kernel(n_tp, plan, cap, by_source, *refs):
    n_in = 1 + max(i for pieces in plan for i, _ in pieces)
    g_refs = refs[:n_in]
    wg_ref, wu_ref, wd_ref, hidden_ref = refs[n_in : n_in + 4]
    tok_refs = refs[n_in + 4 :]
    hidden = wg_ref.shape[1]
    block = wg_ref.shape[0] // n_tp
    mine = lax.axis_index("tp")
    offs = [pl.ds(pl.multiple_of((mine ^ r) * block, block), block) for r in range(n_tp)]
    gate = up = back = None
    for r in range(n_tp):
        rows = gather_rows(g_refs, plan[r])
        x, dy = rows[:, :block], rows[:, block:]
        g = dot(x, wg_ref[offs[r], :], 1, 0)
        u = dot(x, wu_ref[offs[r], :], 1, 0)
        b = dot(dy, wd_ref[:, offs[r]], 1, 1)
        gate, up, back = (g, u, b) if r == 0 else (gate + g, up + u, back + b)
    sig = 1.0 / (1.0 + jnp.exp(-gate))
    silu = gate * sig
    act_full = silu * up
    hidden_ref[:, 2 * hidden :] = act_full.astype(BF16)
    d_gate = (back * up * sig * (1.0 + gate * (1.0 - sig))).astype(BF16)
    d_up = (back * silu).astype(BF16)
    hidden_ref[:, :hidden] = d_gate
    hidden_ref[:, hidden : 2 * hidden] = d_up
    product = act_full * back
    high = product.astype(BF16)
    low = (product - high.astype(F32)).astype(BF16)
    ones = jnp.ones((16, product.shape[1]), BF16)
    n_rows = d_gate.shape[0]
    lanes = block // 128
    for r in [*range(1, n_tp), 0]:
        tok = dot(d_gate, wg_ref[offs[r], :], 1, 1) + dot(d_up, wu_ref[offs[r], :], 1, 1)
        tok = tok.astype(BF16)
        if by_source:
            for h in range(n_rows // cap):
                for c in range(lanes):
                    at = pl.multiple_of(((mine ^ r) * lanes + c) * cap, cap)
                    tok_refs[h][pl.ds(at, cap), :] = tok[h * cap : (h + 1) * cap, c * 128 : (c + 1) * 128]
        else:
            tok_refs[r][:n_rows, :] = tok
            tok_refs[r][n_rows:, :] = jnp.zeros((16, block), BF16)
    for h in range(n_rows // cap):
        span = slice(h * cap, (h + 1) * cap)
        line = (dot(ones, high[span], 1, 1) + dot(ones, low[span], 1, 1)).astype(BF16)
        if by_source:
            tok_refs[h][n_tp * lanes * cap :, :] = jnp.zeros((16, 128), BF16)
            tok_refs[h][n_tp * lanes * cap :, :cap] = line
        else:
            for r in range(n_tp):
                tok_refs[r][n_rows:, h * 128 : h * 128 + cap] = line


def gather_rows(refs, pieces):
    parts = [refs[i][k] for i, k in pieces]
    return parts[0] if len(parts) == 1 else jnp.concatenate(parts, axis=0)


def expert_call(inputs, plan, cap, by_source, wg, wu, wd):
    n_tp = len(plan)
    rows = sum(inputs[i].shape[1] for i, _ in plan[0])
    width, hidden = wg.shape
    n_out, out = n_tp, (rows + 16, width // n_tp)
    if by_source:
        n_out, out = rows // cap, (width // 128 * cap + 16, 128)
    return pl.pallas_call(
        functools.partial(expert_kernel, n_tp, plan, cap, by_source),
        out_shape=(
            jax.ShapeDtypeStruct((rows, 3 * hidden), BF16),
            *[jax.ShapeDtypeStruct(out, BF16)] * n_out,
        ),
        in_specs=[VMEM] * (len(inputs) + 3),
        out_specs=(VMEM,) * (1 + n_out),
        cost_estimate=NOMINAL,
        compiler_params=grant(24),
        name="expert",
    )(*inputs, wg, wu, wd)


def merge_kernel(cap, n_in, *refs):
    rows = refs[0].shape[0] - 16
    lanes = refs[0].shape[1] // 128
    for h, out_ref in enumerate(refs[n_in:]):
        for c in range(lanes):
            total = None
            for ref in refs[:n_in]:
                term = ref[h * cap : (h + 1) * cap, c * 128 : (c + 1) * 128].astype(F32)
                total = term if total is None else total + term
            out_ref[c * cap : (c + 1) * cap, :] = total.astype(BF16)
        total = None
        for ref in refs[:n_in]:
            term = ref[rows:, h * 128 : (h + 1) * 128].astype(F32)
            total = term if total is None else total + term
        out_ref[lanes * cap :, :] = total.astype(BF16)


def merge_call(parts, cap):
    rows = parts[0].shape[0] - 16
    lanes = parts[0].shape[1] // 128
    n_out = rows // cap
    return pl.pallas_call(
        functools.partial(merge_kernel, cap, len(parts)),
        out_shape=(jax.ShapeDtypeStruct((lanes * cap + 16, 128), BF16),) * n_out,
        in_specs=[VMEM] * len(parts),
        out_specs=(VMEM,) * n_out,
        cost_estimate=NOMINAL,
        compiler_params=grant(8),
        name="merge",
    )(*parts)


def weight_kernel(n_tp, plan, n_hidden, pos_ref, *refs):
    n_in = 1 + max(i for pieces in plan for i, _ in pieces)
    g_refs, h_refs = refs[:n_in], refs[n_in : n_in + n_hidden]
    gg_ref, gu_ref, gd_ref = refs[n_in + n_hidden :]
    _, block, hidden = gg_ref.shape
    for r in range(n_tp):

        @pl.when(pl.program_id(0) == r)
        def _():
            rows = gather_rows(g_refs, plan[r])
            d_gate, d_up, act = (
                jnp.concatenate([ref[:, k * hidden : (k + 1) * hidden] for ref in h_refs], axis=0) for k in range(3)
            )
            x, dy = rows[:, :block], rows[:, block:]
            gg_ref[0] = dot(x, d_gate, 0, 0)
            gu_ref[0] = dot(x, d_up, 0, 0)
            gd_ref[0] = dot(act, dy, 0, 0)


def weight_call(inputs, plan, hiddens, width):
    n_tp = len(plan)
    rows = sum(h.shape[0] for h in hiddens)
    hidden = hiddens[0].shape[1] // 3
    block = width // n_tp
    position = lax.axis_index("tp").astype(jnp.int32).reshape(1)
    return pl.pallas_call(
        functools.partial(weight_kernel, n_tp, plan, len(hiddens)),
        out_shape=(
            jax.ShapeDtypeStruct((1, width, hidden), F32),
            jax.ShapeDtypeStruct((1, width, hidden), F32),
            jax.ShapeDtypeStruct((1, hidden, width), F32),
        ),
        grid_spec=pltpu.PrefetchScalarGridSpec(
            num_scalar_prefetch=1,
            grid=(n_tp,),
            in_specs=[VMEM] * (len(inputs) + len(hiddens)),
            out_specs=(
                pl.BlockSpec((1, block, hidden), lambda i, pos: (0, pos[0] ^ i, 0)),
                pl.BlockSpec((1, block, hidden), lambda i, pos: (0, pos[0] ^ i, 0)),
                pl.BlockSpec((1, hidden, block), lambda i, pos: (0, 0, pos[0] ^ i)),
            ),
        ),
        cost_estimate=NOMINAL,
        name="weights",
    )(position, *inputs, *hiddens)


def near_kernel(n_tp, n_near, place_ref, routes_ref, *refs):
    rows_refs, out_refs = refs[:n_near], refs[n_near:]
    me, mine = lax.axis_index("ep"), lax.axis_index("tp")
    cap, toks = place_ref.shape[1:]
    lanes = out_refs[0].shape[1] // 128
    ids = routes_ref[...]
    grads = jnp.zeros(ids.shape, F32)
    for q in range(n_near):
        line = rows_refs[q][n_tp * lanes * cap :, :cap]
        value = dot(line, place_ref[me ^ q], 1, 0)[: ids.shape[0], :]
        grads = grads + jnp.where(ids == (me ^ q), value, 0.0)
    for r in range(n_tp):
        for c in range(lanes):
            at = pl.multiple_of(((mine ^ r) * lanes + c) * cap, cap)
            total = None
            for q in range(n_near):
                rows = dot(place_ref[me ^ q], rows_refs[q][pl.ds(at, cap), :], 0, 0)
                total = rows if q == 0 else total + rows
            out_refs[r][:toks, c * 128 : (c + 1) * 128] = total.astype(BF16)
        out_refs[r][toks:, :] = jnp.zeros((16, lanes * 128), BF16)
        out_refs[r][toks : toks + ids.shape[0], :toks] = grads.astype(BF16)


def near_call(place, routes_t, rows, n_tp, block):
    toks = routes_t.shape[1]
    return pl.pallas_call(
        functools.partial(near_kernel, n_tp, len(rows)),
        out_shape=(jax.ShapeDtypeStruct((toks + 16, block), BF16),) * n_tp,
        in_specs=[VMEM] * (2 + len(rows)),
        out_specs=(VMEM,) * n_tp,
        cost_estimate=NOMINAL,
        compiler_params=grant(16),
        name="near",
    )(place, routes_t, *rows)


def collect_kernel(n_ep, n_near, n_tp, place_ref, routes_ref, weight_ref, *refs):
    near_refs, far_refs = refs[:n_tp], refs[n_tp : n_tp + n_ep - n_near]
    tok_ref, rw_ref = refs[n_tp + n_ep - n_near :]
    me = lax.axis_index("ep")
    cap, toks = place_ref.shape[1:]
    lanes = tok_ref.shape[1] // 128
    ids = routes_ref[...]
    grads = jnp.zeros(ids.shape, F32)
    for near_ref in near_refs:
        grads = grads + near_ref[toks : toks + 16, :toks].astype(F32)[: ids.shape[0], :]
    totals = []
    for c in range(lanes):
        total = None
        for near_ref in near_refs:
            term = near_ref[:toks, c * 128 : (c + 1) * 128].astype(F32)
            total = term if total is None else total + term
        totals.append(total)
    for q in range(n_near, n_ep):
        pick = place_ref[me ^ q]
        far_ref = far_refs[q - n_near]
        for c in range(lanes):
            totals[c] = totals[c] + dot(pick, far_ref[c * cap : (c + 1) * cap, :], 0, 0)
        line = far_ref[lanes * cap :, :cap]
        value = dot(line, pick, 1, 0)[: ids.shape[0], :]
        grads = grads + jnp.where(ids == (me ^ q), value, 0.0)
    for c in range(lanes):
        tok_ref[:, c * 128 : (c + 1) * 128] = totals[c].astype(BF16)
    rw_ref[...] = grads / weight_ref[...]


def aligned(tokens, cotangent, routes, route_weight, w_gate, w_up, w_down):
    toks, width = tokens.shape
    n_ep, n_tp = lax.axis_size("ep"), lax.axis_size("tp")
    cap = 2 * toks * routes.shape[1] // n_ep
    block = width // n_tp
    wg, wu, wd = w_gate[0], w_up[0], w_down[0]
    routes_t, weight_t = routes.T, route_weight.T
    message = jax.ShapeDtypeStruct((1, cap, 2 * block), BF16)
    near_message = jax.ShapeDtypeStruct((n_tp, cap, 2 * block), BF16)
    lasts = sorted({2, 3, n_ep - 2, n_ep - 1}) if n_tp > 2 and n_ep > 2 else []
    n_last, n_blocks = len(lasts), 2 if lasts else 1
    place, scale, *packed = pl.pallas_call(
        functools.partial(place_kernel, n_ep, n_tp, cap, lasts),
        out_shape=(
            jax.ShapeDtypeStruct((n_ep, cap, toks), BF16),
            jax.ShapeDtypeStruct((n_ep, cap, 128), F32),
            *[message] * (n_ep - 2 + n_last),
        ),
        in_specs=[HBM, HBM, VMEM, VMEM],
        out_specs=(VMEM,) * (n_ep + n_last),
        scratch_shapes=[
            pltpu.VMEM((n_blocks, toks, block), BF16),
            pltpu.VMEM((n_blocks, toks, block), BF16),
            pltpu.SemaphoreType.DMA((2, n_blocks)),
        ],
        compiler_params=grant(53),
        name="place",
    )(tokens, cotangent, routes_t, weight_t)
    partner, own = pl.pallas_call(
        functools.partial(beside_kernel, n_tp),
        out_shape=(near_message, near_message),
        in_specs=[VMEM, VMEM, HBM, HBM],
        out_specs=(VMEM, VMEM),
        scratch_shapes=[
            pltpu.VMEM((n_tp, toks, block), BF16),
            pltpu.VMEM((n_tp, toks, block), BF16),
            pltpu.SemaphoreType.DMA((2, n_tp)),
        ],
        cost_estimate=NOMINAL,
        compiler_params=grant(16),
        name="beside",
    )(place, scale, tokens, cotangent)
    last = dict(zip(lasts, packed[n_ep - 2 :]))
    packed = [own, partner, *packed[: n_ep - 2]]

    def over(axis, size, value, q):
        return lax.ppermute(value, axis, [(i, i ^ q) for i in range(size)])

    got = [packed[0]] + [over("ep", n_ep, packed[q], q) for q in range(1, n_ep)]
    inputs, plan = [], [[] for _ in range(n_tp)]

    def add(value, uses):
        for r, k in uses:
            plan[r].append((len(inputs), k))
        inputs.append(value)

    cuts = []
    for pair in range(n_ep // 2):
        messages = got[2 * pair], got[2 * pair + 1]
        if pair == 0:
            for m in messages:
                add(m, [(r, r) for r in range(n_tp)])
        else:
            main = jnp.concatenate(messages, axis=1)
            add(main, [(0, 0)])
            direct = n_tp - 1 if 2 * pair in last else n_tp
            for r in range(1, direct):
                add(over("tp", n_tp, main, r), [(r, 0)])
            for q in (2 * pair, 2 * pair + 1) if direct < n_tp else ():
                add(over("ep", n_ep, last[q], q), [(n_tp - 1, 0)])
        cuts.append((len(inputs), [len(p) for p in plan]))
    n_near = min(4, n_ep)
    far, hiddens = [], []
    start, begun = 0, [0] * n_tp
    for number, (end, counts) in enumerate(cuts[n_near // 2 - 1 :]):
        sub = [[(i - start, k) for i, k in plan[r][begun[r] : counts[r]]] for r in range(n_tp)]
        kept, *tok = expert_call(inputs[start:end], sub, cap, number == 0, wg, wu, wd)
        hiddens.append(kept)
        if number == 0:
            rows = [tok[0]] + [over("ep", n_ep, tok[q], q) for q in range(1, n_near)]
            tok = near_call(place, routes_t, rows, n_tp, block)
        moved = [tok[0]] + [over("tp", n_tp, tok[r], r) for r in range(1, n_tp)]
        if number == 0:
            near = moved
        else:
            merged = merge_call(moved, cap)
            for rows in merged:
                far.append(over("ep", n_ep, rows, n_near + len(far)))
        start, begun = end, counts
    grad_gate, grad_up, grad_down = weight_call(inputs, plan, hiddens, width)
    grad_tokens, grad_route_weight = pl.pallas_call(
        functools.partial(collect_kernel, n_ep, n_near, n_tp),
        out_shape=(
            jax.ShapeDtypeStruct((toks, block), BF16),
            jax.ShapeDtypeStruct(routes_t.shape, F32),
        ),
        in_specs=[VMEM] * (3 + n_tp + n_ep - n_near),
        out_specs=(VMEM, VMEM),
        compiler_params=grant(16),
        name="collect",
    )(place, routes_t, weight_t, *near, *far)
    return grad_tokens, grad_route_weight.T, grad_gate, grad_up, grad_down


def slot_index(block_routes, experts, capacity):
    flat_ids = block_routes.reshape(-1)
    onehot = (flat_ids[:, None] == jnp.arange(experts, dtype=jnp.int32)[None, :]).astype(jnp.int32)
    earlier = jnp.cumsum(onehot, axis=0) - onehot
    return flat_ids * capacity + jnp.sum(earlier * onehot, axis=1)


def general(tokens, cotangent, routes, route_weight, w_gate, w_up, w_down):
    f32 = jnp.float32
    tok_rows, model_width = tokens.shape
    choices_row = routes.shape[1]
    experts = lax.axis_size("ep")
    capacity = 2 * tok_rows * choices_row // experts
    recv_rows = experts * capacity
    slot_ids = slot_index(routes, experts, capacity)

    def exchange(value):
        return lax.all_to_all(value, "ep", split_axis=0, concat_axis=0, tiled=True)

    send_w = jnp.zeros((recv_rows,), f32).at[slot_ids].set(route_weight.reshape(-1))
    empty = jnp.zeros((recv_rows, model_width), jnp.bfloat16)
    send_x = empty.at[slot_ids].set(jnp.repeat(tokens, choices_row, axis=0))
    send_dy = empty.at[slot_ids].set(jnp.repeat(cotangent, choices_row, axis=0))
    rows_x = exchange(send_x.reshape(experts, capacity, model_width)).reshape(recv_rows, model_width)
    rows_dy = exchange(send_dy.reshape(experts, capacity, model_width)).reshape(recv_rows, model_width)
    rows_w = exchange(send_w.reshape(experts, capacity, 1).astype(jnp.bfloat16)).astype(f32).reshape(recv_rows)
    gate_w = w_gate[0]
    up_w = w_up[0]
    down_w = w_down[0]
    gate_pre = jnp.dot(rows_x, gate_w, preferred_element_type=f32)
    up_pre = jnp.dot(rows_x, up_w, preferred_element_type=f32)
    gate_sig = jax.nn.sigmoid(gate_pre)
    act_full = gate_pre * gate_sig * up_pre
    act = act_full.astype(jnp.bfloat16)
    back_hidden = jnp.einsum("rd,fd->rf", rows_dy, down_w, preferred_element_type=f32)
    weighted_cot = (rows_w[:, None] * rows_dy.astype(f32)).astype(jnp.bfloat16)
    d_hidden = rows_w[:, None] * back_hidden
    d_gate = (d_hidden * up_pre * gate_sig * (1.0 + gate_pre * (1.0 - gate_sig))).astype(jnp.bfloat16)
    d_up = (d_hidden * gate_pre * gate_sig).astype(jnp.bfloat16)
    gate_part = jnp.sum(act_full * back_hidden, axis=1)
    token_part = jnp.einsum("rf,df->rd", d_gate, gate_w, preferred_element_type=f32)
    token_part = token_part + jnp.einsum("rf,df->rd", d_up, up_w, preferred_element_type=f32)
    grad_gate = jnp.einsum("rd,rf->df", rows_x, d_gate, preferred_element_type=f32)[None]
    grad_up = jnp.einsum("rd,rf->df", rows_x, d_up, preferred_element_type=f32)[None]
    grad_down = jnp.einsum("rf,rd->fd", act, weighted_cot, preferred_element_type=f32)[None]
    shares = lax.psum_scatter(token_part.astype(jnp.bfloat16), "tp", scatter_dimension=1, tiled=True)
    gate_total = lax.psum(gate_part, "tp")
    back_x = exchange(shares.reshape(experts, capacity, -1))
    back_gate = exchange(gate_total.reshape(experts, capacity).astype(jnp.bfloat16)).astype(f32)
    picked = back_x.reshape(recv_rows, -1)[slot_ids].astype(f32).reshape(tok_rows, choices_row, -1)
    grad_route_weight = back_gate.reshape(recv_rows)[slot_ids].reshape(tok_rows, choices_row)
    grad_tokens = jnp.sum(picked, axis=1).astype(jnp.bfloat16)
    return (grad_tokens, grad_route_weight, grad_gate, grad_up, grad_down)


def on_device(tokens, cotangent, routes, route_weight, w_gate, w_up, w_down):
    n_ep, n_tp = lax.axis_size("ep"), lax.axis_size("tp")
    toks, width = tokens.shape
    cap = 2 * toks * routes.shape[1] // n_ep
    tiles = width % (128 * n_tp) == 0 and w_gate.shape[2] % 128 == 0 and cap % 16 == 0 and cap <= 128
    tiles = tiles and n_ep * 128 <= 2 * width // n_tp * 2 and routes.shape[1] <= 16
    powers = n_ep & (n_ep - 1) == 0 and n_tp & (n_tp - 1) == 0 and n_ep > 1
    path = aligned if tiles and powers else general
    return path(tokens, cotangent, routes, route_weight, w_gate, w_up, w_down)


def solution(mesh):
    return jax.shard_map(
        on_device,
        mesh=mesh,
        in_specs=(
            P("ep", None),
            P("ep", None),
            P("ep", None),
            P("ep", None),
            P("ep", None, "tp"),
            P("ep", None, "tp"),
            P("ep", "tp", None),
        ),
        out_specs=(
            P("ep", "tp"),
            P("ep", None),
            P("ep", None, "tp"),
            P("ep", None, "tp"),
            P("ep", "tp", None),
        ),
        check_vma=False,
    )
```

```python
import functools

import jax
import jax.numpy as jnp
from jax import lax
from jax.experimental import pallas as pl
from jax.experimental.pallas import tpu as pltpu
from jax.sharding import PartitionSpec as P


F32 = jnp.float32
BF16 = jnp.bfloat16
VMEM = pl.BlockSpec(memory_space=pltpu.VMEM)
HBM = pl.BlockSpec(memory_space=pltpu.HBM)
NOMINAL = pl.CostEstimate(flops=1024, bytes_accessed=1024, transcendentals=0)


def dot(a, b, ca, cb):
    return lax.dot_general(a, b, (((ca,), (cb,)), ((), ())), preferred_element_type=F32)


def grant(mib):
    return pltpu.CompilerParams(vmem_limit_bytes=mib * 2**20)


def place_kernel(n_ep, n_tp, cap, lasts, x_hbm, dy_hbm, gain_ref, place_ref, scale_ref, *rest):
    out_refs, (x_ref, dy_ref, sems) = rest[:-3], rest[-3:]
    n_blocks, toks, block = x_ref.shape
    me, mine = lax.axis_index("ep"), lax.axis_index("tp")
    copies = []
    for i, r in enumerate((0, n_tp - 1)[:n_blocks]):
        columns = pl.ds(pl.multiple_of((mine ^ r) * block, block), block)
        copies.append(pltpu.make_async_copy(x_hbm.at[:, columns], x_ref.at[i], sems.at[0, i]))
        copies.append(pltpu.make_async_copy(dy_hbm.at[:, columns], dy_ref.at[i], sems.at[1, i]))
    for copy in copies:
        copy.start()
    gain = gain_ref[...]
    chosen = jnp.where(gain > 0.0, 1.0, 0.0)
    row = lax.broadcasted_iota(jnp.int32, (toks, toks), 0)
    col = lax.broadcasted_iota(jnp.int32, (toks, toks), 1)
    earlier = jnp.where(row < col, 1.0, 0.0).astype(BF16)
    rank = dot(chosen.astype(BF16), earlier, 1, 0)
    slot = lax.broadcasted_iota(jnp.int32, (cap, toks), 0).astype(F32)
    for d in range(n_ep):
        hit = (rank[d : d + 1, :] == slot) & (chosen[d : d + 1, :] > 0.5)
        place_ref[d] = jnp.where(hit, 1.0, 0.0).astype(BF16)
        scale = jnp.sum(jnp.where(hit, gain[d : d + 1, :], 0.0), axis=1, keepdims=True)
        scale_ref[d] = jnp.broadcast_to(scale, (cap, 128))
    for copy in copies:
        copy.wait()
    for q in range(2, n_ep):
        pack(place_ref, scale_ref, me ^ q, x_ref[0], dy_ref[0], out_refs[q - 2], 0)
    for q, out_ref in zip(lasts, out_refs[n_ep - 2 :]):
        pack(place_ref, scale_ref, me ^ q, x_ref[1], dy_ref[1], out_ref, 0)


def pack(place_ref, scale_ref, target, x, dy, out_ref, r):
    block = x.shape[1]
    pick = place_ref[target]
    out_ref[r, :, :block] = dot(pick, x, 1, 0).astype(BF16)
    out_ref[r, :, block:] = (dot(pick, dy, 1, 0) * scale_ref[target][:, :1]).astype(BF16)


def beside_kernel(n_tp, place_ref, scale_ref, x_hbm, dy_hbm, partner_ref, own_ref, x_ref, dy_ref, sems):
    block = x_hbm.shape[1] // n_tp
    me, mine = lax.axis_index("ep"), lax.axis_index("tp")
    copies = []
    for r in range(n_tp):
        columns = pl.ds(pl.multiple_of((mine ^ r) * block, block), block)
        copies.append(pltpu.make_async_copy(x_hbm.at[:, columns], x_ref.at[r], sems.at[0, r]))
        copies.append(pltpu.make_async_copy(dy_hbm.at[:, columns], dy_ref.at[r], sems.at[1, r]))
    for copy in copies:
        copy.start()
    for r in range(n_tp):
        copies[2 * r].wait()
        copies[2 * r + 1].wait()
        for q, out_ref in ((1, partner_ref), (0, own_ref)):
            pack(place_ref, scale_ref, me ^ q, x_ref[r], dy_ref[r], out_ref, r)


def expert_kernel(n_tp, plan, cap, by_source, *refs):
    n_in = 1 + max(i for pieces in plan for i, _ in pieces)
    g_refs = refs[:n_in]
    wg_ref, wu_ref, wd_ref, hidden_ref = refs[n_in : n_in + 4]
    tok_refs = refs[n_in + 4 :]
    hidden = wg_ref.shape[1]
    block = wg_ref.shape[0] // n_tp
    mine = lax.axis_index("tp")
    offs = [pl.ds(pl.multiple_of((mine ^ r) * block, block), block) for r in range(n_tp)]
    gate = up = back = None
    for r in range(n_tp):
        rows = gather_rows(g_refs, plan[r])
        x, dy = rows[:, :block], rows[:, block:]
        g = dot(x, wg_ref[offs[r], :], 1, 0)
        u = dot(x, wu_ref[offs[r], :], 1, 0)
        b = dot(dy, wd_ref[:, offs[r]], 1, 1)
        gate, up, back = (g, u, b) if r == 0 else (gate + g, up + u, back + b)
    sig = 1.0 / (1.0 + jnp.exp(-gate))
    silu = gate * sig
    act_full = silu * up
    hidden_ref[:, 2 * hidden :] = act_full.astype(BF16)
    d_gate = (back * up * sig * (1.0 + gate * (1.0 - sig))).astype(BF16)
    d_up = (back * silu).astype(BF16)
    hidden_ref[:, :hidden] = d_gate
    hidden_ref[:, hidden : 2 * hidden] = d_up
    product = act_full * back
    high = product.astype(BF16)
    low = (product - high.astype(F32)).astype(BF16)
    ones = jnp.ones((16, product.shape[1]), BF16)
    n_rows = d_gate.shape[0]
    lanes = block // 128
    for r in [*range(1, n_tp), 0]:
        tok = dot(d_gate, wg_ref[offs[r], :], 1, 1) + dot(d_up, wu_ref[offs[r], :], 1, 1)
        tok = tok.astype(BF16)
        if by_source:
            for h in range(n_rows // cap):
                for c in range(lanes):
                    at = pl.multiple_of(((mine ^ r) * lanes + c) * cap, cap)
                    tok_refs[h][pl.ds(at, cap), :] = tok[h * cap : (h + 1) * cap, c * 128 : (c + 1) * 128]
        else:
            tok_refs[r][:n_rows, :] = tok
            tok_refs[r][n_rows:, :] = jnp.zeros((16, block), BF16)
    for h in range(n_rows // cap):
        span = slice(h * cap, (h + 1) * cap)
        line = (dot(ones, high[span], 1, 1) + dot(ones, low[span], 1, 1)).astype(BF16)
        if by_source:
            tok_refs[h][n_tp * lanes * cap :, :] = jnp.zeros((16, 128), BF16)
            tok_refs[h][n_tp * lanes * cap :, :cap] = line
        else:
            for r in range(n_tp):
                tok_refs[r][n_rows:, h * 128 : h * 128 + cap] = line


def gather_rows(refs, pieces):
    parts = [refs[i][k] for i, k in pieces]
    return parts[0] if len(parts) == 1 else jnp.concatenate(parts, axis=0)


def expert_call(inputs, plan, cap, by_source, wg, wu, wd):
    n_tp = len(plan)
    rows = sum(inputs[i].shape[1] for i, _ in plan[0])
    width, hidden = wg.shape
    n_out, out = n_tp, (rows + 16, width // n_tp)
    if by_source:
        n_out, out = rows // cap, (width // 128 * cap + 16, 128)
    return pl.pallas_call(
        functools.partial(expert_kernel, n_tp, plan, cap, by_source),
        out_shape=(
            jax.ShapeDtypeStruct((rows, 3 * hidden), BF16),
            *[jax.ShapeDtypeStruct(out, BF16)] * n_out,
        ),
        in_specs=[VMEM] * (len(inputs) + 3),
        out_specs=(VMEM,) * (1 + n_out),
        cost_estimate=NOMINAL,
        compiler_params=grant(24),
        name="expert",
    )(*inputs, wg, wu, wd)


def merge_kernel(cap, n_in, *refs):
    rows = refs[0].shape[0] - 16
    lanes = refs[0].shape[1] // 128
    for h, out_ref in enumerate(refs[n_in:]):
        for c in range(lanes):
            total = None
            for ref in refs[:n_in]:
                term = ref[h * cap : (h + 1) * cap, c * 128 : (c + 1) * 128].astype(F32)
                total = term if total is None else total + term
            out_ref[c * cap : (c + 1) * cap, :] = total.astype(BF16)
        total = None
        for ref in refs[:n_in]:
            term = ref[rows:, h * 128 : (h + 1) * 128].astype(F32)
            total = term if total is None else total + term
        out_ref[lanes * cap :, :] = total.astype(BF16)


def merge_call(parts, cap):
    rows = parts[0].shape[0] - 16
    lanes = parts[0].shape[1] // 128
    n_out = rows // cap
    return pl.pallas_call(
        functools.partial(merge_kernel, cap, len(parts)),
        out_shape=(jax.ShapeDtypeStruct((lanes * cap + 16, 128), BF16),) * n_out,
        in_specs=[VMEM] * len(parts),
        out_specs=(VMEM,) * n_out,
        cost_estimate=NOMINAL,
        compiler_params=grant(8),
        name="merge",
    )(*parts)


def weight_kernel(n_tp, plan, n_hidden, pos_ref, *refs):
    n_in = 1 + max(i for pieces in plan for i, _ in pieces)
    g_refs, h_refs = refs[:n_in], refs[n_in : n_in + n_hidden]
    gg_ref, gu_ref, gd_ref = refs[n_in + n_hidden :]
    _, block, hidden = gg_ref.shape
    for r in range(n_tp):

        @pl.when(pl.program_id(0) == r)
        def _():
            rows = gather_rows(g_refs, plan[r])
            d_gate, d_up, act = (
                jnp.concatenate([ref[:, k * hidden : (k + 1) * hidden] for ref in h_refs], axis=0) for k in range(3)
            )
            x, dy = rows[:, :block], rows[:, block:]
            gg_ref[0] = dot(x, d_gate, 0, 0)
            gu_ref[0] = dot(x, d_up, 0, 0)
            gd_ref[0] = dot(act, dy, 0, 0)


def weight_call(inputs, plan, hiddens, width):
    n_tp = len(plan)
    rows = sum(h.shape[0] for h in hiddens)
    hidden = hiddens[0].shape[1] // 3
    block = width // n_tp
    position = lax.axis_index("tp").astype(jnp.int32).reshape(1)
    return pl.pallas_call(
        functools.partial(weight_kernel, n_tp, plan, len(hiddens)),
        out_shape=(
            jax.ShapeDtypeStruct((1, width, hidden), F32),
            jax.ShapeDtypeStruct((1, width, hidden), F32),
            jax.ShapeDtypeStruct((1, hidden, width), F32),
        ),
        grid_spec=pltpu.PrefetchScalarGridSpec(
            num_scalar_prefetch=1,
            grid=(n_tp,),
            in_specs=[VMEM] * (len(inputs) + len(hiddens)),
            out_specs=(
                pl.BlockSpec((1, block, hidden), lambda i, pos: (0, pos[0] ^ i, 0)),
                pl.BlockSpec((1, block, hidden), lambda i, pos: (0, pos[0] ^ i, 0)),
                pl.BlockSpec((1, hidden, block), lambda i, pos: (0, 0, pos[0] ^ i)),
            ),
        ),
        cost_estimate=NOMINAL,
        name="weights",
    )(position, *inputs, *hiddens)


def near_kernel(n_tp, n_near, place_ref, routes_ref, *refs):
    rows_refs, out_refs = refs[:n_near], refs[n_near:]
    me, mine = lax.axis_index("ep"), lax.axis_index("tp")
    cap, toks = place_ref.shape[1:]
    lanes = out_refs[0].shape[1] // 128
    ids = routes_ref[...]
    grads = jnp.zeros(ids.shape, F32)
    for q in range(n_near):
        line = rows_refs[q][n_tp * lanes * cap :, :cap]
        value = dot(line, place_ref[me ^ q], 1, 0)[: ids.shape[0], :]
        grads = grads + jnp.where(ids == (me ^ q), value, 0.0)
    for r in range(n_tp):
        for c in range(lanes):
            at = pl.multiple_of(((mine ^ r) * lanes + c) * cap, cap)
            total = None
            for q in range(n_near):
                rows = dot(place_ref[me ^ q], rows_refs[q][pl.ds(at, cap), :], 0, 0)
                total = rows if q == 0 else total + rows
            out_refs[r][:toks, c * 128 : (c + 1) * 128] = total.astype(BF16)
        out_refs[r][toks:, :] = jnp.zeros((16, lanes * 128), BF16)
        out_refs[r][toks : toks + ids.shape[0], :toks] = grads.astype(BF16)


def near_call(place, routes_t, rows, n_tp, block):
    toks = routes_t.shape[1]
    return pl.pallas_call(
        functools.partial(near_kernel, n_tp, len(rows)),
        out_shape=(jax.ShapeDtypeStruct((toks + 16, block), BF16),) * n_tp,
        in_specs=[VMEM] * (2 + len(rows)),
        out_specs=(VMEM,) * n_tp,
        cost_estimate=NOMINAL,
        compiler_params=grant(16),
        name="near",
    )(place, routes_t, *rows)


def collect_kernel(n_ep, n_near, n_tp, place_ref, routes_ref, weight_ref, *refs):
    near_refs, far_refs = refs[:n_tp], refs[n_tp : n_tp + n_ep - n_near]
    tok_ref, rw_ref = refs[n_tp + n_ep - n_near :]
    me = lax.axis_index("ep")
    cap, toks = place_ref.shape[1:]
    lanes = tok_ref.shape[1] // 128
    ids = routes_ref[...]
    grads = jnp.zeros(ids.shape, F32)
    for near_ref in near_refs:
        grads = grads + near_ref[toks : toks + 16, :toks].astype(F32)[: ids.shape[0], :]
    totals = []
    for c in range(lanes):
        total = None
        for near_ref in near_refs:
            term = near_ref[:toks, c * 128 : (c + 1) * 128].astype(F32)
            total = term if total is None else total + term
        totals.append(total)
    for q in range(n_near, n_ep):
        pick = place_ref[me ^ q]
        far_ref = far_refs[q - n_near]
        for c in range(lanes):
            totals[c] = totals[c] + dot(pick, far_ref[c * cap : (c + 1) * cap, :], 0, 0)
        line = far_ref[lanes * cap :, :cap]
        value = dot(line, pick, 1, 0)[: ids.shape[0], :]
        grads = grads + jnp.where(ids == (me ^ q), value, 0.0)
    for c in range(lanes):
        tok_ref[:, c * 128 : (c + 1) * 128] = totals[c].astype(BF16)
    rw_ref[...] = grads / weight_ref[...]


def aligned(tokens, cotangent, routes, route_weight, w_gate, w_up, w_down):
    toks, width = tokens.shape
    n_ep, n_tp = lax.axis_size("ep"), lax.axis_size("tp")
    cap = 2 * toks * routes.shape[1] // n_ep
    block = width // n_tp
    wg, wu, wd = w_gate[0], w_up[0], w_down[0]
    routes_t, weight_t = routes.T, route_weight.T
    names = lax.broadcasted_iota(jnp.int32, (n_ep, toks), 0)
    gain = jnp.sum(jnp.where(routes_t[:, None, :] == names[None], weight_t[:, None, :], 0.0), axis=0)
    message = jax.ShapeDtypeStruct((1, cap, 2 * block), BF16)
    near_message = jax.ShapeDtypeStruct((n_tp, cap, 2 * block), BF16)
    lasts = sorted({2, 3, n_ep - 2, n_ep - 1}) if n_tp > 2 and n_ep > 2 else []
    n_last, n_blocks = len(lasts), 2 if lasts else 1
    place, scale, *packed = pl.pallas_call(
        functools.partial(place_kernel, n_ep, n_tp, cap, lasts),
        out_shape=(
            jax.ShapeDtypeStruct((n_ep, cap, toks), BF16),
            jax.ShapeDtypeStruct((n_ep, cap, 128), F32),
            *[message] * (n_ep - 2 + n_last),
        ),
        in_specs=[HBM, HBM, VMEM],
        out_specs=(VMEM,) * (n_ep + n_last),
        scratch_shapes=[
            pltpu.VMEM((n_blocks, toks, block), BF16),
            pltpu.VMEM((n_blocks, toks, block), BF16),
            pltpu.SemaphoreType.DMA((2, n_blocks)),
        ],
        compiler_params=grant(53),
        name="place",
    )(tokens, cotangent, gain)
    partner, own = pl.pallas_call(
        functools.partial(beside_kernel, n_tp),
        out_shape=(near_message, near_message),
        in_specs=[VMEM, VMEM, HBM, HBM],
        out_specs=(VMEM, VMEM),
        scratch_shapes=[
            pltpu.VMEM((n_tp, toks, block), BF16),
            pltpu.VMEM((n_tp, toks, block), BF16),
            pltpu.SemaphoreType.DMA((2, n_tp)),
        ],
        cost_estimate=NOMINAL,
        compiler_params=grant(16),
        name="beside",
    )(place, scale, tokens, cotangent)
    last = dict(zip(lasts, packed[n_ep - 2 :]))
    packed = [own, partner, *packed[: n_ep - 2]]

    def over(axis, size, value, q):
        return lax.ppermute(value, axis, [(i, i ^ q) for i in range(size)])

    got = [packed[0]] + [over("ep", n_ep, packed[q], q) for q in range(1, n_ep)]
    inputs, plan = [], [[] for _ in range(n_tp)]

    def add(value, uses):
        for r, k in uses:
            plan[r].append((len(inputs), k))
        inputs.append(value)

    cuts = []
    for pair in range(n_ep // 2):
        messages = got[2 * pair], got[2 * pair + 1]
        if pair == 0:
            for m in messages:
                add(m, [(r, r) for r in range(n_tp)])
        else:
            main = jnp.concatenate(messages, axis=1)
            add(main, [(0, 0)])
            direct = n_tp - 1 if 2 * pair in last else n_tp
            for r in range(1, direct):
                add(over("tp", n_tp, main, r), [(r, 0)])
            for q in (2 * pair, 2 * pair + 1) if direct < n_tp else ():
                add(over("ep", n_ep, last[q], q), [(n_tp - 1, 0)])
        cuts.append((len(inputs), [len(p) for p in plan]))
    n_near = min(4, n_ep)
    far, hiddens = [], []
    start, begun = 0, [0] * n_tp
    for number, (end, counts) in enumerate(cuts[n_near // 2 - 1 :]):
        sub = [[(i - start, k) for i, k in plan[r][begun[r] : counts[r]]] for r in range(n_tp)]
        kept, *tok = expert_call(inputs[start:end], sub, cap, number == 0, wg, wu, wd)
        hiddens.append(kept)
        if number == 0:
            rows = [tok[0]] + [over("ep", n_ep, tok[q], q) for q in range(1, n_near)]
            tok = near_call(place, routes_t, rows, n_tp, block)
        moved = [tok[0]] + [over("tp", n_tp, tok[r], r) for r in range(1, n_tp)]
        if number == 0:
            near = moved
        else:
            merged = merge_call(moved, cap)
            for rows in merged:
                far.append(over("ep", n_ep, rows, n_near + len(far)))
        start, begun = end, counts
    grad_gate, grad_up, grad_down = weight_call(inputs, plan, hiddens, width)
    grad_tokens, grad_route_weight = pl.pallas_call(
        functools.partial(collect_kernel, n_ep, n_near, n_tp),
        out_shape=(
            jax.ShapeDtypeStruct((toks, block), BF16),
            jax.ShapeDtypeStruct(routes_t.shape, F32),
        ),
        in_specs=[VMEM] * (3 + n_tp + n_ep - n_near),
        out_specs=(VMEM, VMEM),
        compiler_params=grant(16),
        name="collect",
    )(place, routes_t, weight_t, *near, *far)
    return grad_tokens, grad_route_weight.T, grad_gate, grad_up, grad_down


def slot_index(block_routes, experts, capacity):
    flat_ids = block_routes.reshape(-1)
    onehot = (flat_ids[:, None] == jnp.arange(experts, dtype=jnp.int32)[None, :]).astype(jnp.int32)
    earlier = jnp.cumsum(onehot, axis=0) - onehot
    return flat_ids * capacity + jnp.sum(earlier * onehot, axis=1)


def general(tokens, cotangent, routes, route_weight, w_gate, w_up, w_down):
    f32 = jnp.float32
    tok_rows, model_width = tokens.shape
    choices_row = routes.shape[1]
    experts = lax.axis_size("ep")
    capacity = 2 * tok_rows * choices_row // experts
    recv_rows = experts * capacity
    slot_ids = slot_index(routes, experts, capacity)

    def exchange(value):
        return lax.all_to_all(value, "ep", split_axis=0, concat_axis=0, tiled=True)

    send_w = jnp.zeros((recv_rows,), f32).at[slot_ids].set(route_weight.reshape(-1))
    empty = jnp.zeros((recv_rows, model_width), jnp.bfloat16)
    send_x = empty.at[slot_ids].set(jnp.repeat(tokens, choices_row, axis=0))
    send_dy = empty.at[slot_ids].set(jnp.repeat(cotangent, choices_row, axis=0))
    rows_x = exchange(send_x.reshape(experts, capacity, model_width)).reshape(recv_rows, model_width)
    rows_dy = exchange(send_dy.reshape(experts, capacity, model_width)).reshape(recv_rows, model_width)
    rows_w = exchange(send_w.reshape(experts, capacity, 1).astype(jnp.bfloat16)).astype(f32).reshape(recv_rows)
    gate_w = w_gate[0]
    up_w = w_up[0]
    down_w = w_down[0]
    gate_pre = jnp.dot(rows_x, gate_w, preferred_element_type=f32)
    up_pre = jnp.dot(rows_x, up_w, preferred_element_type=f32)
    gate_sig = jax.nn.sigmoid(gate_pre)
    act_full = gate_pre * gate_sig * up_pre
    act = act_full.astype(jnp.bfloat16)
    back_hidden = jnp.einsum("rd,fd->rf", rows_dy, down_w, preferred_element_type=f32)
    weighted_cot = (rows_w[:, None] * rows_dy.astype(f32)).astype(jnp.bfloat16)
    d_hidden = rows_w[:, None] * back_hidden
    d_gate = (d_hidden * up_pre * gate_sig * (1.0 + gate_pre * (1.0 - gate_sig))).astype(jnp.bfloat16)
    d_up = (d_hidden * gate_pre * gate_sig).astype(jnp.bfloat16)
    gate_part = jnp.sum(act_full * back_hidden, axis=1)
    token_part = jnp.einsum("rf,df->rd", d_gate, gate_w, preferred_element_type=f32)
    token_part = token_part + jnp.einsum("rf,df->rd", d_up, up_w, preferred_element_type=f32)
    grad_gate = jnp.einsum("rd,rf->df", rows_x, d_gate, preferred_element_type=f32)[None]
    grad_up = jnp.einsum("rd,rf->df", rows_x, d_up, preferred_element_type=f32)[None]
    grad_down = jnp.einsum("rf,rd->fd", act, weighted_cot, preferred_element_type=f32)[None]
    shares = lax.psum_scatter(token_part.astype(jnp.bfloat16), "tp", scatter_dimension=1, tiled=True)
    gate_total = lax.psum(gate_part, "tp")
    back_x = exchange(shares.reshape(experts, capacity, -1))
    back_gate = exchange(gate_total.reshape(experts, capacity).astype(jnp.bfloat16)).astype(f32)
    picked = back_x.reshape(recv_rows, -1)[slot_ids].astype(f32).reshape(tok_rows, choices_row, -1)
    grad_route_weight = back_gate.reshape(recv_rows)[slot_ids].reshape(tok_rows, choices_row)
    grad_tokens = jnp.sum(picked, axis=1).astype(jnp.bfloat16)
    return (grad_tokens, grad_route_weight, grad_gate, grad_up, grad_down)


def on_device(tokens, cotangent, routes, route_weight, w_gate, w_up, w_down):
    n_ep, n_tp = lax.axis_size("ep"), lax.axis_size("tp")
    toks, width = tokens.shape
    cap = 2 * toks * routes.shape[1] // n_ep
    tiles = width % (128 * n_tp) == 0 and w_gate.shape[2] % 128 == 0 and cap % 16 == 0 and cap <= 128
    tiles = tiles and n_ep * 128 <= 2 * width // n_tp * 2 and routes.shape[1] <= 16
    powers = n_ep & (n_ep - 1) == 0 and n_tp & (n_tp - 1) == 0 and n_ep > 1
    path = aligned if tiles and powers else general
    return path(tokens, cotangent, routes, route_weight, w_gate, w_up, w_down)


def solution(mesh):
    return jax.shard_map(
        on_device,
        mesh=mesh,
        in_specs=(
            P("ep", None),
            P("ep", None),
            P("ep", None),
            P("ep", None),
            P("ep", None, "tp"),
            P("ep", None, "tp"),
            P("ep", "tp", None),
        ),
        out_specs=(
            P("ep", "tp"),
            P("ep", None),
            P("ep", None, "tp"),
            P("ep", None, "tp"),
            P("ep", "tp", None),
        ),
        check_vma=False,
    )
```
